32 devices in a mesh: fs: 8 (over z, x), tp: 4 (over y, core).
Axes of the slice: x: 2, y: 2, z: 4, core: 2. Of those that a mesh axis runs over, the one named last changes fastest.
Arguments:
- tokens: bfloat16 [1024, 2048], P('fs'), may hold values from -6 to 6
- route_ids: int32 [1024, 2], P('fs'), may hold values from 0 to 15, as said below
- route_weights: float32 [1024, 2], P('fs'), may hold values from 0.05 to 0.6
- norm_gain: float32 [2048], P('fs'), may hold values from 0.1 to 1.9
- gate_weight: float32 [16, 2048, 1024], P(None, 'fs', 'tp'), may hold values from -6 to 6
- up_weight: float32 [16, 2048, 1024], P(None, 'fs', 'tp'), may hold values from -6 to 6
- down_weight: float32 [16, 2048, 1024], P(None, 'fs', 'tp'), may hold values from -6 to 6
Outputs:
- gate_served: bfloat16 [16, 2048, 1024], P('fs', None, 'tp')
- up_served: bfloat16 [16, 2048, 1024], P('fs', None, 'tp')
- down_served: bfloat16 [16, 2048, 1024], P('fs', None, 'tp')
- combined: bfloat16 [1024, 2048], P('fs', 'tp')
The draws below stay inside these ranges and needn't reach their ends.
Inputs may be any that keep to these rules, and one draw needn't show every extreme that they name: `route_ids`: each row names 2 different experts of one group, numbers g * 4 to g * 4 + 3 for some g. In each aligned block of 128 rows (the rows of one index of fs) no expert is named by more than 32 rows, and some experts are named by exactly 32 rows in every block.
All inputs are finite; a program needn't handle non-finite values.
Results may differ from the reference program's by a relative error of at most 0.015.
Values may be sent and summed in bfloat16 or wider, within the bound.
A program may use at most 64 MiB of HBM per device.

```python
import jax
import jax.numpy as jnp
from jax import lax

D = 2048
H = 1024
GROUPS = 4
TOP = 2
TOK_DEV = 128
EXPERTS = 16
CAP = 32
TOKENS = 1024
N_TP = 4


def shuffle_table(table_key):
    return jax.random.permutation(table_key, EXPERTS // GROUPS)


def draw_route_ids(key, part):
    per_group = EXPERTS // GROUPS
    heavy_group = jax.random.randint(jax.random.fold_in(key, 11), (), 0, GROUPS)

    def one_block(block_number):
        block_key = jax.random.fold_in(jax.random.fold_in(key, 23), block_number)
        shuffled = jax.random.permutation(jax.random.fold_in(block_key, 1), TOK_DEV)
        other_shift = jax.random.randint(jax.random.fold_in(block_key, 2), (TOK_DEV,), 1, GROUPS)
        ranked = jnp.zeros((TOK_DEV,), jnp.int32).at[shuffled].set(jnp.arange(TOK_DEV, dtype=jnp.int32))
        group_ids = jnp.where(ranked < TOK_DEV // 2, heavy_group, (heavy_group + other_shift) % GROUPS)
        onehot = (group_ids[:, None] == jnp.arange(GROUPS, dtype=jnp.int32)[None, :]).astype(jnp.int32)
        rank_in = jnp.sum((jnp.cumsum(onehot, axis=0) - onehot) * onehot, axis=1)
        offsets = jax.random.randint(jax.random.fold_in(block_key, 3), (GROUPS,), 0, per_group)
        tables = jax.vmap(shuffle_table)(jax.random.split(jax.random.fold_in(block_key, 4), GROUPS))
        position = 2 * rank_in + jnp.sum(onehot * offsets[None, :], axis=1)
        first_slot = position % per_group
        second_slot = (position + 1) % per_group
        row_table = tables[group_ids]
        pick_first = jnp.take_along_axis(row_table, first_slot[:, None], axis=1)
        pick_second = jnp.take_along_axis(row_table, second_slot[:, None], axis=1)
        return jnp.concatenate([pick_first, pick_second], axis=1) + group_ids[:, None] * per_group
    blocks = jax.vmap(one_block)(jnp.arange(TOKENS // TOK_DEV, dtype=jnp.int32))
    return blocks.reshape(TOKENS, TOP).astype(jnp.int32)


def block_levels(stream_key, dims, cuts, least, largest):
    factor_of = 1.0
    for dim, blocks in cuts:
        draws = jax.random.uniform(jax.random.fold_in(jax.random.fold_in(stream_key, 6), dim), (blocks,), jnp.float32, least / len(cuts), largest / len(cuts))
        factor_of = factor_of * jnp.repeat(jnp.exp(draws), dims[dim] // blocks).reshape((-1,) + (1,) * (len(dims) - 1 - dim))
    return factor_of


def bell_draw(stream_key, shape, deviation, reach, cuts=(), kind=jnp.bfloat16):
    array = jax.random.normal(stream_key, shape, jnp.float32) * deviation
    if len(cuts) > 0:
        array = block_levels(stream_key, shape, cuts, -0.22, 0.18) * array
    return jnp.clip(array, min=-reach, max=reach).astype(kind)


def setup_inputs(seed: int = 0) -> dict:
    key_list = jax.random.split(jax.random.key(seed), 8)
    return {
        "tokens": bell_draw(key_list[0], (TOKENS, D), 1.0, 6.0, ((0, 8),)),
        "route_ids": draw_route_ids(jax.random.fold_in(key_list[7], 71), 0),
        "route_weights": jnp.clip(0.05 + 0.55 * jax.random.uniform(key_list[2], (TOKENS, TOP), jnp.float32) ** block_levels(key_list[2], (TOKENS, TOP), ((0, 8),), -0.2, 0.2), 0.05, 0.6),
        "norm_gain": jnp.clip(1.0 + 0.18 * jax.random.normal(key_list[3], (D,), jnp.float32), 0.1, 1.9),
        "gate_weight": bell_draw(key_list[4], (EXPERTS, D, H), 1.0, 6.0, ((1, 8), (2, 4)), jnp.float32),
        "up_weight": bell_draw(key_list[5], (EXPERTS, D, H), 1.0, 6.0, ((1, 8), (2, 4)), jnp.float32),
        "down_weight": bell_draw(key_list[6], (EXPERTS, D, H), 1.0, 6.0, ((1, 8), (2, 4)), jnp.float32),
    }


epsilon = 1e-06

def slot_positions(route_ids):
    blocked = route_ids.reshape(TOKENS // TOK_DEV, TOK_DEV * TOP)
    onehot = (blocked[:, :, None] == jnp.arange(EXPERTS, dtype=jnp.int32)[None, None, :]).astype(jnp.int32)
    earlier = jnp.cumsum(onehot, axis=1) - onehot
    return lax.optimization_barrier(jnp.sum(earlier * onehot, axis=2)).reshape(TOKENS, TOP).astype(jnp.int32)

def reference(tokens, route_ids, route_weights, norm_gain, gate_weight, up_weight, down_weight):
    scaling = norm_gain[:, None]
    gate_served = (scaling * gate_weight).astype(jnp.bfloat16)
    up_served = (scaling * up_weight).astype(jnp.bfloat16)
    down_served = down_weight.astype(jnp.bfloat16)
    widened = tokens.astype(jnp.float32)
    normed = (widened * lax.rsqrt(lax.optimization_barrier(jnp.mean(widened * widened, axis=1, keepdims=True)) + epsilon)).astype(jnp.bfloat16)
    block_index = (jnp.arange(TOKENS, dtype=jnp.int32) // TOK_DEV)[:, None]
    slot_index = (block_index * CAP + slot_positions(route_ids)).astype(jnp.int32)
    slot_rows = TOKENS // TOK_DEV * CAP
    token_of = jnp.broadcast_to(jnp.arange(TOKENS, dtype=jnp.int32)[:, None], (TOKENS, TOP))
    row_owner = jnp.zeros((EXPERTS, slot_rows), jnp.int32).at[route_ids, slot_index].set(token_of)

    def expert(operands):
        gate_one, up_one, down_one, owners = operands
        inputs = normed[owners]
        gate_pre = jnp.dot(inputs, gate_one, preferred_element_type=jnp.float32) * D ** (-0.5)
        up_pre = jnp.dot(inputs, up_one, preferred_element_type=jnp.float32) * D ** (-0.5)
        hidden = (jax.nn.silu(gate_pre) * up_pre).astype(jnp.bfloat16)
        blocks_h = hidden.astype(jnp.float32).reshape(slot_rows, N_TP, H // N_TP)
        blocks_d = down_one.astype(jnp.float32).reshape(D, N_TP, H // N_TP)
        partial_value = (jnp.einsum('rtj,dtj->trd', blocks_h, blocks_d) * H ** (-0.5)).astype(jnp.bfloat16)
        return lax.optimization_barrier(jnp.sum(partial_value.astype(jnp.float32), axis=0)).astype(jnp.bfloat16)
    expert_outs = lax.map(expert, (gate_served, up_served, down_served, row_owner))
    picked = expert_outs[route_ids, slot_index].astype(jnp.float32)
    combined = lax.optimization_barrier(jnp.sum(route_weights[:, :, None] * picked, axis=1))
    return (gate_served, up_served, down_served, combined.astype(jnp.bfloat16))
```

```python
import functools

import jax
import jax.numpy as jnp
from jax import lax
from jax.experimental import pallas as pl
from jax.experimental.pallas import tpu as pltpu
from jax.sharding import PartitionSpec as P

GROUPS = 4
EPSILON = 1e-06
MESH = pl.DeviceIdType.MESH
LAG = 2
LANES = 128
F32, BF16, I32 = jnp.float32, jnp.bfloat16, jnp.int32


def matmul(a, b, contract=((1,), (0,))):
    return lax.dot_general(a, b, (contract, ((), ())), preferred_element_type=F32)


def placement(ids_t, per_group, slots):
    n_tok = ids_t.shape[1]
    slot = lax.broadcasted_iota(I32, (GROUPS * slots, n_tok), 0)
    member = ids_t[0:1, :] // per_group == slot // slots
    earlier = (
        lax.broadcasted_iota(I32, (n_tok, n_tok), 0) < lax.broadcasted_iota(I32, (n_tok, n_tok), 1)
    )
    place = matmul(member.astype(F32).astype(BF16), earlier.astype(F32).astype(BF16))
    return (member & (place.astype(I32) == slot % slots)).astype(F32).astype(BF16)


def each(first, last, action):
    def go(k, carry):
        action(k)
        return carry
    lax.fori_loop(first, last, go, 0)


def kernel(
    nf, nt,
    tokens, ids_t, weights_t, gain, gate, up, down,
    gate_out, up_out, down_out, ret,
    wf, ws, xs, vs, xr, vr, wc, hs, ps, pr, qs, qr, rs,
    load_sem, wsend, wrecv, xsend, xrecv, vsend, vrecv, msend, mrecv, nsend, nrecv, gsend, grecv,
    psend, precv, qsend, qrecv, rsend, rrecv,
):
    f, t = lax.axis_index("fs"), lax.axis_index("tp")
    experts, rows, hidden = gate.shape
    n_tok, d_model = tokens.shape
    per = experts // nf
    cols = d_model // nt
    width = nf // GROUPS
    slots = xs.shape[1]
    per_group = experts // GROUPS
    plane = width * slots
    parts = max(1, rows // LANES)
    part = rows // parts
    joint = max(1, LANES // rows)
    pieces = d_model // LANES
    per_owner = cols // LANES
    g, m = f // width, lax.rem(f, width)
    served = (gate_out, up_out, down_out)

    def target(k):
        return lax.rem(f + k, nf)

    def source(k):
        return lax.rem(f - k + nf, nf)

    def other(k):
        return lax.rem(t + k, nt)

    def mate(k):
        return lax.rem(m + k, width)

    def group(k):
        return lax.rem(g + k, GROUPS)

    def span(start, size):
        return pl.ds(pl.multiple_of(start * size, size), size)

    def loads(a, k):
        p = target(k)
        return pltpu.make_async_copy(
            (gate, up, down)[a].at[pl.ds(p * per, per)],
            wf.at[a % 2, pl.ds(p * per, per)],
            load_sem.at[a, k],
        )

    def remote(src, dst, send, recv, device):
        return pltpu.make_async_remote_copy(
            src_ref=src, dst_ref=dst, send_sem=send, recv_sem=recv,
            device_id=device, device_id_type=MESH,
        )

    def weight_copy(a, p, src):
        return remote(
            ws.at[a, pl.ds(p * per, per)],
            served[a].at[:, span(src, rows), :],
            wsend.at[a, 0, p], wrecv.at[a, 0, src], {"fs": p},
        )

    def down_copy(h, p, src):
        return remote(
            ws.at[2, pl.ds(p * per, per), span(h, part), :],
            down_out.at[:, span(src * parts + h, part), :],
            wsend.at[2, h, p], wrecv.at[2, h, src], {"fs": p},
        )

    def token_copy(to, src):
        return remote(
            xs.at[to], xr.at[t, src, m], xsend.at[to], xrecv.at[src], {"fs": to * width + m}
        )

    def share_copy(to, src):
        return remote(vs.at[to], vr.at[src, m], vsend.at[to], vrecv.at[src], {"fs": to * width + m})

    def token_relay(to, src):
        return remote(
            xr.at[t, :, src], xr.at[t, :, src], msend.at[to], mrecv.at[src], {"fs": g * width + to}
        )

    def share_relay(to, src):
        return remote(
            vr.at[:, src], vr.at[:, src], nsend.at[to], nrecv.at[src], {"fs": g * width + to}
        )

    def gather_copy(to, src):
        return remote(xr.at[src], xr.at[src], gsend.at[to], grecv.at[src], {"tp": to})

    def partial_copy(c, to, src):
        return remote(
            ps.at[c, span(to, plane), :], pr.at[src, c],
            psend.at[c, to], precv.at[c, src], {"tp": to},
        )

    def mate_copy(c, to, src):
        return remote(
            qs.at[c, to], qr.at[src, c], qsend.at[c, to], qrecv.at[c, src], {"fs": g * width + to}
        )

    def return_copy(c, to_fs, to_tp, src):
        i = lax.rem(c, per_owner)
        return remote(
            rs.at[c], ret.at[i, span(src, slots), :],
            rsend.at[c], rrecv.at[src, i], {"fs": to_fs, "tp": to_tp},
        )

    each(1, nf, lambda k: loads(0, k).start())
    loads(0, 0).start()

    barrier = pltpu.get_barrier_semaphore()
    each(1, nf, lambda k: pl.semaphore_signal(
        barrier, inc=1, device_id={"fs": target(k)}, device_id_type=MESH))
    each(1, nt, lambda k: pl.semaphore_signal(
        barrier, inc=1, device_id={"tp": other(k)}, device_id_type=MESH))
    pl.semaphore_wait(barrier, nf + nt - 2)

    square = lax.broadcasted_iota(I32, (rows, rows), 0) == lax.broadcasted_iota(I32, (rows, rows), 1)
    gain_column = jnp.sum(jnp.where(square, gain[...], 0.0), axis=1, keepdims=True)

    def converted(a, n):
        value = wf[a % 2, n]
        if a < 2:
            value = value * gain_column
        return value.astype(BF16)

    def send_weights(a):
        def load_next(k):
            if a < 2:
                loads(a + 1, k).start()

        def one(k):
            p = target(k)
            loads(a, k).wait()
            load_next(k)
            for e in range(per):
                ws[a, p * per + e] = converted(a, p * per + e)
            if a < 2:
                weight_copy(a, p, f).start()
            else:
                down_copy(0, p, f).start()
        each(1, nf, one)
        loads(a, 0).wait()
        load_next(0)
        for e in range(per):
            served[a][e, span(f, rows), :] = converted(a, f * per + e)
        if a == 2:
            for h in range(1, parts):
                each(1, nf, lambda k: down_copy(h, target(k), f).start())

    send_weights(0)

    wide = tokens[...].astype(F32)
    scale = lax.rsqrt(jnp.mean(wide * wide, axis=1, keepdims=True) + EPSILON)
    own = tokens[:, span(t, cols)].astype(F32)
    normed = (own * scale).astype(BF16)
    chosen = placement(ids_t, per_group, slots)
    xs[...] = matmul(chosen, normed).reshape(GROUPS, slots, cols).astype(BF16)
    vs[...] = jnp.zeros(vs.shape, F32)
    row = lax.broadcasted_iota(I32, (vs.shape[1], n_tok), 0)
    for i in range(GROUPS):
        value = jnp.zeros((vs.shape[1], n_tok), F32)
        for r in range(ids_t.shape[0]):
            value += jnp.where(
                (row < per_group) & (row + i * per_group == ids_t[r:r + 1, :]),
                weights_t[r:r + 1, :], 0.0)
        high = value.astype(BF16)
        low = (value - high.astype(F32)).astype(BF16)
        here = chosen[i * slots:(i + 1) * slots]
        vs[i, :, 0:slots] = (
            matmul(high, here, ((1,), (1,))) + matmul(low, here, ((1,), (1,))))

    def dispatch(k):
        token_copy(group(k), g).start()
        share_copy(group(k), g).start()
    each(1, GROUPS, dispatch)
    xr[t, g, m] = xs[g]
    vr[g, m] = vs[g]

    send_weights(1)
    send_weights(2)

    def arrive(k):
        token_copy(g, group(k)).wait_recv()
        share_copy(g, group(k)).wait_recv()
    each(1, GROUPS, arrive)

    def relay(k):
        token_relay(mate(k), m).start()
        share_relay(mate(k), m).start()
    each(1, width, relay)

    def relayed(k):
        token_relay(m, mate(k)).wait_recv()
        share_relay(m, mate(k)).wait_recv()
    each(1, width, relayed)
    each(1, nt, lambda k: gather_copy(other(k), t).start())

    eye = lax.broadcasted_iota(I32, (slots, n_tok), 0) == lax.broadcasted_iota(I32, (slots, n_tok), 1)

    def shares(n):
        i, w = n // width, lax.rem(n, width)
        for e in range(per):
            line = vr[i, w, pl.ds(m * per + e, 1), :]
            column = jnp.sum(jnp.where(eye, line, 0.0), axis=1, keepdims=True)
            wc[e, span(n, slots), :] = jnp.broadcast_to(column, (slots, LANES))
    each(0, nf, shares)

    each(1, nt, lambda k: gather_copy(t, other(k)).wait_recv())

    def product(a, e, i):
        total = jnp.zeros((plane, hidden), F32)
        for o in range(nt):
            left = xr[o, i].reshape(plane, cols)
            total += matmul(left, served[a][e, o * cols:(o + 1) * cols, :])
        return total * d_model ** (-0.5)

    each(1, nf, lambda k: weight_copy(0, f, source(k)).wait_recv())
    each(1, nf, lambda k: weight_copy(1, f, source(k)).wait_recv())

    def activate(i):
        for e in range(per):
            v = product(0, e, i)
            value = v / (1.0 + jnp.exp(-v)) * product(1, e, i)
            value = value * wc[e, span(i, plane), 0:1]
            hs[span(i, plane), e * hidden:(e + 1) * hidden] = value.astype(BF16)
    each(0, GROUPS, activate)

    hidden_scale = (hidden * nt) ** (-0.5)
    blocks = pieces // parts
    first_block = g * width // joint

    def piece_at(n):
        return (first_block ^ lax.rem(n, blocks)) * parts + n // blocks

    def multiply(n):
        c = piece_at(n)
        h = lax.rem(c, parts)
        for q in range(joint):
            s = c // parts * joint + q

            @pl.when(s != f)
            def _():
                down_copy(h, f, s).wait_recv()
        value = jnp.zeros((nf * slots, LANES), F32)
        for e in range(per):
            value += matmul(
                hs[:, e * hidden:(e + 1) * hidden], down_out[e, span(c, LANES), :], ((1,), (1,)))
        ps[c] = (value * hidden_scale).astype(BF16)
        each(1, nt, lambda k: partial_copy(c, other(k), t).start())

    def reduce(n):
        c = piece_at(n)
        each(1, nt, lambda k: partial_copy(c, t, other(k)).wait_recv())
        total = ps[c, span(t, plane), :].astype(F32)
        for k in range(1, nt):
            total += pr[other(k), c].astype(F32)
        qs[c] = total.astype(BF16).reshape(width, slots, LANES)
        each(1, width, lambda k: mate_copy(c, mate(k), m).start())

    def give_back(n):
        c = piece_at(n)
        each(1, width, lambda k: mate_copy(c, m, mate(k)).wait_recv())
        total = qs[c, m].astype(F32)
        for k in range(1, width):
            total += qr[mate(k), c].astype(F32)
        rs[c] = total.astype(BF16)
        owner = c // per_owner
        local = (t == g) & (owner == t)

        @pl.when(local)
        def _():
            ret[lax.rem(c, per_owner), span(g, slots), :] = rs[c]

        @pl.when(jnp.logical_not(local))
        def _():
            return_copy(c, t * width + m, owner, g).start()

    def step(n):
        @pl.when(n < pieces)
        def _():
            multiply(n)

        @pl.when((n >= LAG) & (n < pieces + LAG))
        def _():
            reduce(n - LAG)

        @pl.when(n >= 2 * LAG)
        def _():
            give_back(n - 2 * LAG)
    each(0, pieces + 2 * LAG, step)

    def returned(n):
        i, src = lax.rem(n, per_owner), n // per_owner

        @pl.when(jnp.logical_not((src == g) & (t == g)))
        def _():
            return_copy(t * per_owner + i, f, t, src).wait_recv()
    each(0, GROUPS * per_owner, returned)

    def drain(k):
        p = target(k)
        for a in range(2):
            weight_copy(a, p, f).wait_send()
        for h in range(parts):
            down_copy(h, p, f).wait_send()
    each(1, nf, drain)

    def drain_tokens(k):
        token_copy(group(k), g).wait_send()
        share_copy(group(k), g).wait_send()
    each(1, GROUPS, drain_tokens)

    def drain_relay(k):
        token_relay(mate(k), m).wait_send()
        share_relay(mate(k), m).wait_send()
    each(1, width, drain_relay)
    each(1, nt, lambda k: gather_copy(other(k), t).wait_send())

    def drain_piece(c):
        each(1, nt, lambda k: partial_copy(c, other(k), t).wait_send())
        each(1, width, lambda k: mate_copy(c, mate(k), m).wait_send())
        owner = c // per_owner

        @pl.when(jnp.logical_not((t == g) & (owner == t)))
        def _():
            return_copy(c, t * width + m, owner, g).wait_send()
    each(0, pieces, drain_piece)


def finish_kernel(ids_t, ret, gate, up, down, gate_out, up_out, down_out, combined, sem, *, per_group):
    outs = [
        pltpu.make_async_copy(source, target, sem.at[a])
        for a, (source, target) in enumerate(((gate, gate_out), (up, up_out), (down, down_out)))
    ]
    for copy in outs:
        copy.start()
    chunks, slots, width = ret.shape
    chosen = placement(ids_t, per_group, slots // GROUPS)
    for i in range(chunks):
        value = matmul(chosen, ret[i], ((0,), (0,)))
        combined[:, i * width:(i + 1) * width] = value.astype(BF16)
    for copy in outs:
        copy.wait()


def body(nf, nt, tokens, route_ids, route_weights, norm_gain, gate_weight, up_weight, down_weight):
    experts, rows, hidden = gate_weight.shape
    n_tok, d_model = tokens.shape
    per = experts // nf
    cols = d_model // nt
    slots = n_tok // route_ids.shape[1]
    width = nf // GROUPS
    per_group = experts // GROUPS
    lines = max(8, per_group)
    parts = max(1, rows // LANES)
    pieces = d_model // LANES
    per_owner = cols // LANES
    shape = (per, nf * rows, hidden)
    vmem, anywhere = pl.BlockSpec(memory_space=pltpu.VMEM), pl.BlockSpec(memory_space=pl.ANY)
    dma = pltpu.SemaphoreType.DMA
    ids_t, weights_t = route_ids.T, route_weights.T
    *served, ret = pl.pallas_call(
        functools.partial(kernel, nf, nt),
        out_shape=[pltpu.VMEM(shape, BF16)] * 3
        + [pltpu.VMEM((per_owner, GROUPS * slots, LANES), BF16)],
        in_specs=[vmem] * 4 + [anywhere] * 3,
        out_specs=[vmem] * 4,
        scratch_shapes=[
            pltpu.VMEM((2, experts, rows, hidden), F32),
            pltpu.VMEM((3, experts, rows, hidden), BF16),
            pltpu.VMEM((GROUPS, slots, cols), BF16),
            pltpu.VMEM((GROUPS, lines, n_tok), F32),
            pltpu.VMEM((nt, GROUPS, width, slots, cols), BF16),
            pltpu.VMEM((GROUPS, width, lines, n_tok), F32),
            pltpu.VMEM((per, nf * slots, LANES), F32),
            pltpu.VMEM((nf * slots, per * hidden), BF16),
            pltpu.VMEM((pieces, nf * slots, LANES), BF16),
            pltpu.VMEM((nt, pieces, width * slots, LANES), BF16),
            pltpu.VMEM((pieces, width, slots, LANES), BF16),
            pltpu.VMEM((width, pieces, slots, LANES), BF16),
            pltpu.VMEM((pieces, slots, LANES), BF16),
            dma((3, nf)),
            dma((3, parts, nf)), dma((3, parts, nf)),
            dma((GROUPS,)), dma((GROUPS,)),
            dma((GROUPS,)), dma((GROUPS,)),
            dma((width,)), dma((width,)),
            dma((width,)), dma((width,)),
            dma((nt,)), dma((nt,)),
            dma((pieces, nt)), dma((pieces, nt)),
            dma((pieces, width)), dma((pieces, width)),
            dma((pieces,)), dma((GROUPS, per_owner)),
        ],
        compiler_params=pltpu.CompilerParams(
            collective_id=0, has_side_effects=True, vmem_limit_bytes=54 * 1024 * 1024
        ),
    )(tokens, ids_t, weights_t, norm_gain[None, :], gate_weight, up_weight, down_weight)
    out = jax.ShapeDtypeStruct(shape, BF16)
    return pl.pallas_call(
        functools.partial(finish_kernel, per_group=per_group),
        out_shape=(out, out, out, jax.ShapeDtypeStruct((n_tok, cols), BF16)),
        in_specs=[vmem] * 5,
        out_specs=(anywhere, anywhere, anywhere, vmem),
        scratch_shapes=[dma((3,))],
        compiler_params=pltpu.CompilerParams(vmem_limit_bytes=16 * 1024 * 1024),
    )(ids_t, ret, *served)


def solution(mesh):
    split = P(None, "fs", "tp")
    served = P("fs", None, "tp")
    return jax.shard_map(
        functools.partial(body, mesh.shape["fs"], mesh.shape["tp"]),
        mesh=mesh,
        in_specs=(P("fs", None), P("fs", None), P("fs", None), P("fs"), split, split, split),
        out_specs=(served, served, served, P("fs", "tp")),
        check_vma=False,
    )
```

```python
import functools

import jax
import jax.numpy as jnp
from jax import lax
from jax.experimental import pallas as pl
from jax.experimental.pallas import tpu as pltpu
from jax.sharding import PartitionSpec as P

GROUPS = 4
EPSILON = 1e-06
MESH = pl.DeviceIdType.MESH
PAIR_LAG, CREW_LAG = 1, 3
LANES = 128
F32, BF16, I32 = jnp.float32, jnp.bfloat16, jnp.int32


def matmul(a, b, contract=((1,), (0,))):
    return lax.dot_general(a, b, (contract, ((), ())), preferred_element_type=F32)


def placement(ids_t, per_group, slots):
    n_tok = ids_t.shape[1]
    slot = lax.broadcasted_iota(I32, (GROUPS * slots, n_tok), 0)
    member = ids_t[0:1, :] // per_group == slot // slots
    earlier = (
        lax.broadcasted_iota(I32, (n_tok, n_tok), 0) < lax.broadcasted_iota(I32, (n_tok, n_tok), 1)
    )
    place = matmul(member.astype(F32).astype(BF16), earlier.astype(F32).astype(BF16))
    return (member & (place.astype(I32) == slot % slots)).astype(F32).astype(BF16)


def each(first, last, action):
    def go(k, carry):
        action(k)
        return carry
    lax.fori_loop(first, last, go, 0)


def kernel(
    nf, nt,
    tokens, ids_t, weights_t, gain, gate, up, down,
    gate_out, up_out, down_out, ret,
    wf, ws, xs, vs, xr, vr, wc, hs, ps, pr, qs, qr, rs,
    load_sem, wsend, wrecv, drecv, xsem, vsem, msem, nsem, gsem, psend, precv, qsend, qrecv, rsem,
):
    f, t = lax.axis_index("fs"), lax.axis_index("tp")
    experts, rows, hidden = gate.shape
    n_tok, d_model = tokens.shape
    per = experts // nf
    cols = d_model // nt
    width = nf // GROUPS
    slots = n_tok // ids_t.shape[0]
    split = nt // GROUPS
    share = slots // split
    per_group = experts // GROUPS
    plane = width * share
    parts = max(1, rows // LANES)
    part = rows // parts
    joint = max(1, LANES // rows)
    pieces = d_model // LANES
    per_owner = cols // LANES
    g, m = f // width, lax.rem(f, width)
    shift = t // 2 + nt // 2 * lax.rem(t, 2)
    home, rest = shift // split, lax.rem(shift, split)
    crews = nt // 2 * width
    served = (gate_out, up_out, down_out)

    def target(k):
        return lax.rem(jnp.where(f < nf // 2, f + k, f + nf - k), nf)

    def other(k):
        return lax.rem(t + k, nt)

    def mate(k):
        return lax.rem(m + k, width)

    def group(k):
        return lax.rem(g + k, GROUPS)

    def span(start, size):
        return pl.ds(pl.multiple_of(start * size, size), size)

    def loads(a, k):
        p = target(k)
        return pltpu.make_async_copy(
            (gate, up, down)[a].at[pl.ds(p * per, per)],
            wf.at[a % 2, pl.ds(p * per, per)],
            load_sem.at[k],
        )

    def remote(src, dst, send, recv, device):
        return pltpu.make_async_remote_copy(
            src_ref=src, dst_ref=dst, send_sem=send, recv_sem=recv,
            device_id=device, device_id_type=MESH,
        )

    def settle(ref, sem):
        pltpu.make_async_copy(ref, ref, sem).wait()

    def weight_copy(a, p, src):
        return remote(
            ws.at[a, pl.ds(p * per, per)],
            served[a].at[:, span(src, rows), :],
            wsend.at[a], wrecv.at[a], {"fs": p},
        )

    def down_copy(h, p, src):
        return remote(
            ws.at[2, pl.ds(p * per, per), span(h, part), :],
            down_out.at[:, span(src * parts + h, part), :],
            wsend.at[2], drecv.at[h, src], {"fs": p},
        )

    def token_copy(to, src):
        return remote(
            xs.at[to], xr.at[t, pl.ds(src * split, split), m], xsem.at[0], xsem.at[1], {"fs": to * width + m}
        )

    def share_copy(to, src):
        return remote(vs.at[to], vr.at[src, m], vsem.at[0], vsem.at[1], {"fs": to * width + m})

    def token_relay(to, src):
        return remote(
            xr.at[t, :, src], xr.at[t, :, src], msem.at[0], msem.at[1], {"fs": g * width + to}
        )

    def share_relay(to, src):
        return remote(
            vr.at[:, src], vr.at[:, src], nsem.at[0], nsem.at[1], {"fs": g * width + to}
        )

    def gather_copy(to, src):
        return remote(xr.at[src], xr.at[src], gsem.at[0], gsem.at[1], {"tp": to})

    def partial_copy(c, to):
        return remote(
            ps.at[c, lax.rem(to, 2)], pr.at[c], psend, precv.at[c], {"tp": t // 2 * 2 + lax.rem(to, 2)}
        )

    def crew(k):
        return lax.rem(t // 2 * width + m + k, crews)

    def crew_copy(c, to, src):
        return remote(
            qs.at[c, to], qr.at[src, c], qsend, qrecv.at[c],
            {"fs": g * width + lax.rem(to, width), "tp": to // width * 2 + lax.rem(t, 2)},
        )

    def return_copy(c, to_fs, to_tp, src):
        i = lax.rem(c, per_owner)
        return remote(
            rs.at[c], ret.at[i, span(src, share), :],
            rsem.at[0], rsem.at[1], {"fs": to_fs, "tp": to_tp},
        )

    each(1, nf, lambda k: loads(0, k).start())
    loads(0, 0).start()

    barrier = pltpu.get_barrier_semaphore()
    each(1, nf, lambda k: pl.semaphore_signal(
        barrier, inc=1, device_id={"fs": target(k)}, device_id_type=MESH))
    each(1, nt, lambda k: pl.semaphore_signal(
        barrier, inc=1, device_id={"tp": other(k)}, device_id_type=MESH))
    wide = tokens[...].astype(F32)
    scale = lax.rsqrt(jnp.mean(wide * wide, axis=1, keepdims=True) + EPSILON)
    own = tokens[:, span(t, cols)].astype(F32)
    normed = (own * scale).astype(BF16)
    chosen = placement(ids_t, per_group, slots)
    xs[...] = matmul(chosen, normed).reshape(GROUPS, split, share, cols).astype(BF16)
    vs[...] = jnp.zeros(vs.shape, F32)
    row = lax.broadcasted_iota(I32, (vs.shape[1], n_tok), 0)
    for i in range(GROUPS):
        value = jnp.zeros((vs.shape[1], n_tok), F32)
        for r in range(ids_t.shape[0]):
            value += jnp.where(
                (row < per_group) & (row + i * per_group == ids_t[r:r + 1, :]),
                weights_t[r:r + 1, :], 0.0)
        high = value.astype(BF16)
        low = (value - high.astype(F32)).astype(BF16)
        here = chosen[i * slots:(i + 1) * slots]
        vs[i, :, 0:slots] = (
            matmul(high, here, ((1,), (1,))) + matmul(low, here, ((1,), (1,))))

    with jax.named_scope('barrier'):
        pl.semaphore_wait(barrier, nf + nt - 2)

    def dispatch(k):
        token_copy(group(k), g).start()
        share_copy(group(k), g).start()
    each(1, GROUPS, dispatch)
    for q in range(split):
        xr[t, g * split + q, m] = xs[g, q]
    vr[g, m] = vs[g]

    square = lax.broadcasted_iota(I32, (rows, rows), 0) == lax.broadcasted_iota(I32, (rows, rows), 1)
    gain_column = jnp.sum(jnp.where(square, gain[...], 0.0), axis=1, keepdims=True)

    def converted(a, n):
        value = wf[a % 2, n]
        if a < 2:
            value = value * gain_column
        return value.astype(BF16)

    def send_weights(a):
        def load_next(k):
            if a < 2:
                loads(a + 1, k).start()

        def one(k):
            p = target(k)
            loads(a, k).wait()
            load_next(k)
            for e in range(per):
                ws[a, p * per + e] = converted(a, p * per + e)
            if a < 2:
                weight_copy(a, p, f).start()
        each(1, nf, one)
        loads(a, 0).wait()
        load_next(0)
        for e in range(per):
            served[a][e, span(f, rows), :] = converted(a, f * per + e)

    def send_down():
        for h in range(parts):
            each(1, nf, lambda k: down_copy(h, target(k), f).start())

    with jax.named_scope('send0'):
        send_weights(0)

    with jax.named_scope('send1'):
        send_weights(1)
    with jax.named_scope('send2'):
        send_weights(2)
    outer = (g == 0) | (g == GROUPS - 1)
    pl.when(jnp.logical_not(outer))(send_down)

    with jax.named_scope('arrive'):
        settle(xs.at[0:GROUPS - 1], xsem.at[1])
        settle(vs.at[0:GROUPS - 1], vsem.at[1])

    def relay(k):
        token_relay(mate(k), m).start()
        share_relay(mate(k), m).start()
    each(1, width, relay)

    with jax.named_scope('relayed'):
        settle(xr.at[t, :, 0:width - 1], msem.at[1])
        settle(vr.at[:, 0:width - 1], nsem.at[1])
    each(1, nt, lambda k: gather_copy(other(k), t).start())

    lane = lax.broadcasted_iota(I32, (share, n_tok), 1) - lax.broadcasted_iota(I32, (share, n_tok), 0)

    def shares(n):
        i, w = n // width, lax.rem(n, width)
        eye = lane == lax.rem(i, split) * share
        for e in range(per):
            line = vr[i // split, w, pl.ds(m * per + e, 1), :]
            column = jnp.sum(jnp.where(eye, line, 0.0), axis=1, keepdims=True)
            wc[e, span(n, share), :] = jnp.broadcast_to(column, (share, LANES))
    each(0, nt * width, shares)

    with jax.named_scope('gather'):
        settle(xr.at[0:nt - 1], gsem.at[1])

    def product(a, e, i):
        total = jnp.zeros((plane, hidden), F32)
        for o in range(nt):
            left = xr[o, i].reshape(plane, cols)
            total += matmul(left, served[a][e, o * cols:(o + 1) * cols, :])
        return total * d_model ** (-0.5)

    with jax.named_scope('wait_gate'):
        settle(ws.at[0, 0:experts - per], wrecv.at[0])
    with jax.named_scope('wait_up'):
        settle(ws.at[1, 0:experts - per], wrecv.at[1])

    def activate(i):
        for e in range(per):
            v = product(0, e, i)
            value = v / (1.0 + jnp.exp(-v)) * product(1, e, i)
            value = value * wc[e, span(i, plane), 0:1]
            hs[span(i, plane), e * hidden:(e + 1) * hidden] = value.astype(BF16)
    pl.when(outer)(send_down)
    with jax.named_scope('activate'):
        each(0, nt, activate)

    hidden_scale = (hidden * nt) ** (-0.5)
    blocks = pieces // parts
    quarter = pieces // GROUPS
    wide_blocks = blocks // GROUPS
    low = g < GROUPS // 2

    def piece_at(n):
        i, r = n // quarter, lax.rem(n, quarter)
        far = jnp.where(low, GROUPS + 1 - i, i - 2)
        z = jnp.where(i < 2, g ^ i, far)
        return (z * wide_blocks + lax.rem(r, wide_blocks)) * parts + r // wide_blocks

    def multiply(n):
        c = piece_at(n)
        h = lax.rem(c, parts)
        for q in range(joint):
            s = c // parts * joint + q

            @pl.when(s != f)
            def _():
                with jax.named_scope('wait_piece'):
                    down_copy(h, f, s).wait_recv()
        value = jnp.zeros((nt * plane, LANES), F32)
        for e in range(per):
            value += matmul(
                hs[:, e * hidden:(e + 1) * hidden], down_out[e, span(c, LANES), :], ((1,), (1,)))
        ps[c] = (value * hidden_scale).astype(BF16).reshape(2, nt // 2, plane, LANES)
        partial_copy(c, t + 1).start()

    def reduce(n):
        c = piece_at(n)
        with jax.named_scope('wait_partial'):
            partial_copy(c, t).wait_recv()
        total = ps[c, lax.rem(t, 2)].astype(F32) + pr[c].astype(F32)
        qs[c] = total.astype(BF16).reshape(crews, share, LANES)
        each(1, crews, lambda k: crew_copy(c, crew(k), crew(0)).start())

    def give_back(n):
        c = piece_at(n)
        with jax.named_scope('wait_mate'):
            settle(qs.at[c, 0:crews - 1], qrecv.at[c])
        total = qs[c, crew(0)].astype(F32)
        for k in range(1, crews):
            total += qr[crew(k), c].astype(F32)
        rs[c] = total.astype(BF16)
        owner = c // per_owner
        local = (home == g) & (owner == t)

        @pl.when(local)
        def _():
            ret[lax.rem(c, per_owner), span(g * split + rest, share), :] = rs[c]

        @pl.when(jnp.logical_not(local))
        def _():
            return_copy(c, home * width + m, owner, g * split + rest).start()

    def step(n):
        @pl.when(n < pieces)
        def _():
            multiply(n)

        @pl.when((n >= PAIR_LAG) & (n < pieces + PAIR_LAG))
        def _():
            reduce(n - PAIR_LAG)

        @pl.when(n >= CREW_LAG)
        def _():
            give_back(n - CREW_LAG)
    each(0, pieces + CREW_LAG, step)

    own_share = pieces - per_owner

    @pl.when(home == g)
    def _():
        settle(ret.at[:, 0:GROUPS * slots - share], rsem.at[1])
        settle(rs.at[0:own_share], rsem.at[0])

    @pl.when(home != g)
    def _():
        settle(ret, rsem.at[1])
        settle(rs, rsem.at[0])

    for a in range(3):
        settle(ws.at[a, 0:experts - per], wsend.at[a])
    settle(xs.at[0:GROUPS - 1], xsem.at[0])
    settle(vs.at[0:GROUPS - 1], vsem.at[0])
    settle(xr.at[t, :, 0:width - 1], msem.at[0])
    settle(vr.at[:, 0:width - 1], nsem.at[0])
    settle(xr.at[0:nt - 1], gsem.at[0])
    settle(pr, psend)
    settle(qs.at[:, 0:crews - 1], qsend)


def finish_kernel(ids_t, ret, gate, up, down, gate_out, up_out, down_out, combined, sem, *, per_group):
    outs = [
        pltpu.make_async_copy(source, target, sem.at[a])
        for a, (source, target) in enumerate(((gate, gate_out), (up, up_out), (down, down_out)))
    ]
    for copy in outs:
        copy.start()
    chunks, slots, width = ret.shape
    chosen = placement(ids_t, per_group, slots // GROUPS)
    for i in range(chunks):
        value = matmul(chosen, ret[i], ((0,), (0,)))
        combined[:, i * width:(i + 1) * width] = value.astype(BF16)
    for copy in outs:
        copy.wait()


def body(nf, nt, tokens, route_ids, route_weights, norm_gain, gate_weight, up_weight, down_weight):
    experts, rows, hidden = gate_weight.shape
    n_tok, d_model = tokens.shape
    per = experts // nf
    cols = d_model // nt
    slots = n_tok // route_ids.shape[1]
    width = nf // GROUPS
    per_group = experts // GROUPS
    lines = max(8, per_group)
    crews = nt // 2 * width
    split = nt // GROUPS
    share = slots // split
    parts = max(1, rows // LANES)
    pieces = d_model // LANES
    per_owner = cols // LANES
    shape = (per, nf * rows, hidden)
    vmem, anywhere = pl.BlockSpec(memory_space=pltpu.VMEM), pl.BlockSpec(memory_space=pl.ANY)
    dma = pltpu.SemaphoreType.DMA
    ids_t, weights_t = route_ids.T, route_weights.T
    *served, ret = pl.pallas_call(
        functools.partial(kernel, nf, nt),
        out_shape=[pltpu.VMEM(shape, BF16)] * 3
        + [pltpu.VMEM((per_owner, GROUPS * slots, LANES), BF16)],
        in_specs=[vmem] * 4 + [anywhere] * 3,
        out_specs=[vmem] * 4,
        scratch_shapes=[
            pltpu.VMEM((2, experts, rows, hidden), F32),
            pltpu.VMEM((3, experts, rows, hidden), BF16),
            pltpu.VMEM((GROUPS, split, share, cols), BF16),
            pltpu.VMEM((GROUPS, lines, n_tok), F32),
            pltpu.VMEM((nt, nt, width, share, cols), BF16),
            pltpu.VMEM((GROUPS, width, lines, n_tok), F32),
            pltpu.VMEM((per, nf * slots, LANES), F32),
            pltpu.VMEM((nf * slots, per * hidden), BF16),
            pltpu.VMEM((pieces, 2, nt // 2, width * share, LANES), BF16),
            pltpu.VMEM((pieces, nt // 2, width * share, LANES), BF16),
            pltpu.VMEM((pieces, crews, share, LANES), BF16),
            pltpu.VMEM((crews, pieces, share, LANES), BF16),
            pltpu.VMEM((pieces, share, LANES), BF16),
            dma((nf,)), dma((3,)), dma((2,)), dma((parts, nf)),
            dma((2,)), dma((2,)), dma((2,)), dma((2,)), dma((2,)),
            dma, dma((pieces,)), dma, dma((pieces,)), dma((2,)),
        ],
        compiler_params=pltpu.CompilerParams(
            collective_id=0, has_side_effects=True, vmem_limit_bytes=54 * 1024 * 1024
        ),
    )(tokens, ids_t, weights_t, norm_gain[None, :], gate_weight, up_weight, down_weight)
    out = jax.ShapeDtypeStruct(shape, BF16)
    return pl.pallas_call(
        functools.partial(finish_kernel, per_group=per_group),
        out_shape=(out, out, out, jax.ShapeDtypeStruct((n_tok, cols), BF16)),
        in_specs=[vmem] * 5,
        out_specs=(anywhere, anywhere, anywhere, vmem),
        scratch_shapes=[dma((3,))],
        compiler_params=pltpu.CompilerParams(vmem_limit_bytes=16 * 1024 * 1024),
    )(ids_t, ret, *served)


def solution(mesh):
    split = P(None, "fs", "tp")
    served = P("fs", None, "tp")
    return jax.shard_map(
        functools.partial(body, mesh.shape["fs"], mesh.shape["tp"]),
        mesh=mesh,
        in_specs=(P("fs", None), P("fs", None), P("fs", None), P("fs"), split, split, split),
        out_specs=(served, served, served, P("fs", "tp")),
        check_vma=False,
    )
```

```python
import functools

import jax
import jax.numpy as jnp
from jax import lax
from jax.experimental import pallas as pl
from jax.experimental.pallas import tpu as pltpu
from jax.sharding import PartitionSpec as P

GROUPS = 4
EPSILON = 1e-06
MESH = pl.DeviceIdType.MESH
PAIR_LAG, CREW_LAG = 1, 3
LANES = 128
F32, BF16, I32 = jnp.float32, jnp.bfloat16, jnp.int32


def matmul(a, b, contract=((1,), (0,))):
    return lax.dot_general(a, b, (contract, ((), ())), preferred_element_type=F32)


def placement(ids_t, per_group, slots):
    n_tok = ids_t.shape[1]
    slot = lax.broadcasted_iota(I32, (GROUPS * slots, n_tok), 0)
    member = ids_t[0:1, :] // per_group == slot // slots
    earlier = (
        lax.broadcasted_iota(I32, (n_tok, n_tok), 0) < lax.broadcasted_iota(I32, (n_tok, n_tok), 1)
    )
    place = matmul(member.astype(F32).astype(BF16), earlier.astype(F32).astype(BF16))
    return (member & (place.astype(I32) == slot % slots)).astype(F32).astype(BF16)


def each(first, last, action):
    def go(k, carry):
        action(k)
        return carry
    lax.fori_loop(first, last, go, 0)


def kernel(
    nf, nt,
    tokens_in, ids_in, weights_in, gain_in, gate, up, down,
    gate_out, up_out, down_out, ret,
    tokens, ids_t, weights_t, gain,
    wf, ws, xs, vs, xr, vr, wc, hs, ps, pr, qs, qr, rs,
    in_sem, load_sem, wsend, wrecv, drecv, xsem, vsem, msem, nsem, gsem, psend, precv, qsend, qrecv, rsem,
):
    f, t = lax.axis_index("fs"), lax.axis_index("tp")
    experts, rows, hidden = gate.shape
    n_tok, d_model = tokens.shape
    per = experts // nf
    cols = d_model // nt
    width = nf // GROUPS
    slots = n_tok // ids_t.shape[0]
    split = nt // GROUPS
    share = slots // split
    per_group = experts // GROUPS
    plane = width * share
    parts = max(1, rows // LANES)
    part = rows // parts
    joint = max(1, LANES // rows)
    pieces = d_model // LANES
    per_owner = cols // LANES
    g, m = f // width, lax.rem(f, width)
    shift = t // 2 + nt // 2 * lax.rem(t, 2)
    home, rest = shift // split, lax.rem(shift, split)
    crews = nt // 2 * width
    served = (gate_out, up_out, down_out)

    def target(k):
        return lax.rem(jnp.where(f < nf // 2, f + k, f + nf - k), nf)

    def other(k):
        return lax.rem(t + k, nt)

    def mate(k):
        return lax.rem(m + k, width)

    def group(k):
        return lax.rem(g + k, GROUPS)

    def span(start, size):
        return pl.ds(pl.multiple_of(start * size, size), size)

    def loads(a, k):
        p = target(k)
        return pltpu.make_async_copy(
            (gate, up, down)[a].at[pl.ds(p * per, per)],
            wf.at[a % 2, pl.ds(p * per, per)],
            load_sem.at[k],
        )

    def remote(src, dst, send, recv, device):
        return pltpu.make_async_remote_copy(
            src_ref=src, dst_ref=dst, send_sem=send, recv_sem=recv,
            device_id=device, device_id_type=MESH,
        )

    def settle(ref, sem):
        pltpu.make_async_copy(ref, ref, sem).wait()

    def weight_copy(a, p, src):
        return remote(
            ws.at[a, pl.ds(p * per, per)],
            served[a].at[:, span(src, rows), :],
            wsend.at[a], wrecv.at[a], {"fs": p},
        )

    def down_copy(h, p, src):
        return remote(
            ws.at[2, pl.ds(p * per, per), span(h, part), :],
            down_out.at[:, span(src * parts + h, part), :],
            wsend.at[2], drecv.at[h, src], {"fs": p},
        )

    def token_copy(to, src):
        return remote(
            xs.at[to], xr.at[t, pl.ds(src * split, split), m], xsem.at[0], xsem.at[1], {"fs": to * width + m}
        )

    def share_copy(to, src):
        return remote(vs.at[to], vr.at[src, m], vsem.at[0], vsem.at[1], {"fs": to * width + m})

    def token_relay(to, src):
        return remote(
            xr.at[t, :, src], xr.at[t, :, src], msem.at[0], msem.at[1], {"fs": g * width + to}
        )

    def share_relay(to, src):
        return remote(
            vr.at[:, src], vr.at[:, src], nsem.at[0], nsem.at[1], {"fs": g * width + to}
        )

    def gather_copy(to, src):
        return remote(xr.at[src], xr.at[src], gsem.at[0], gsem.at[1], {"tp": to})

    def partial_copy(c, to):
        return remote(
            ps.at[c, lax.rem(to, 2)], pr.at[c], psend, precv.at[c], {"tp": t // 2 * 2 + lax.rem(to, 2)}
        )

    def crew(k):
        return lax.rem(t // 2 * width + m + k, crews)

    def crew_copy(c, to, src):
        return remote(
            qs.at[c, to], qr.at[src, c], qsend, qrecv.at[c],
            {"fs": g * width + lax.rem(to, width), "tp": to // width * 2 + lax.rem(t, 2)},
        )

    def return_copy(c, to_fs, to_tp, src):
        i = lax.rem(c, per_owner)
        return remote(
            rs.at[c], ret.at[i, span(src, share), :],
            rsem.at[0], rsem.at[1], {"fs": to_fs, "tp": to_tp},
        )

    barrier = pltpu.get_barrier_semaphore()
    each(1, nf, lambda k: pl.semaphore_signal(
        barrier, inc=1, device_id={"fs": target(k)}, device_id_type=MESH))
    each(1, nt, lambda k: pl.semaphore_signal(
        barrier, inc=1, device_id={"tp": other(k)}, device_id_type=MESH))
    inputs = [
        pltpu.make_async_copy(src, dst, in_sem.at[i])
        for i, (src, dst) in enumerate((
            (tokens_in, tokens), (ids_in, ids_t), (weights_in, weights_t), (gain_in, gain)))
    ]
    for copy in inputs:
        copy.start()
    each(1, nf, lambda k: loads(0, k).start())
    loads(0, 0).start()
    for copy in inputs:
        copy.wait()
    wide = tokens[...].astype(F32)
    scale = lax.rsqrt(jnp.mean(wide * wide, axis=1, keepdims=True) + EPSILON)
    own = tokens[:, span(t, cols)].astype(F32)
    normed = (own * scale).astype(BF16)
    chosen = placement(ids_t, per_group, slots)
    xs[...] = matmul(chosen, normed).reshape(GROUPS, split, share, cols).astype(BF16)
    vs[...] = jnp.zeros(vs.shape, F32)
    row = lax.broadcasted_iota(I32, (vs.shape[1], n_tok), 0)
    for i in range(GROUPS):
        value = jnp.zeros((vs.shape[1], n_tok), F32)
        for r in range(ids_t.shape[0]):
            value += jnp.where(
                (row < per_group) & (row + i * per_group == ids_t[r:r + 1, :]),
                weights_t[r:r + 1, :], 0.0)
        high = value.astype(BF16)
        low = (value - high.astype(F32)).astype(BF16)
        here = chosen[i * slots:(i + 1) * slots]
        vs[i, :, 0:slots] = (
            matmul(high, here, ((1,), (1,))) + matmul(low, here, ((1,), (1,))))

    with jax.named_scope('barrier'):
        pl.semaphore_wait(barrier, nf + nt - 2)

    def dispatch(k):
        token_copy(group(k), g).start()
        share_copy(group(k), g).start()
    each(1, GROUPS, dispatch)
    for q in range(split):
        xr[t, g * split + q, m] = xs[g, q]
    vr[g, m] = vs[g]

    square = lax.broadcasted_iota(I32, (rows, rows), 0) == lax.broadcasted_iota(I32, (rows, rows), 1)
    gain_column = jnp.sum(jnp.where(square, gain[...], 0.0), axis=1, keepdims=True)

    def converted(a, n):
        value = wf[a % 2, n]
        if a < 2:
            value = value * gain_column
        return value.astype(BF16)

    def send_weights(a):
        def load_next(k):
            if a < 2:
                loads(a + 1, k).start()

        def one(k):
            p = target(k)
            loads(a, k).wait()
            load_next(k)
            for e in range(per):
                ws[a, p * per + e] = converted(a, p * per + e)
            if a < 2:
                weight_copy(a, p, f).start()
        each(1, nf, one)
        loads(a, 0).wait()
        load_next(0)
        for e in range(per):
            served[a][e, span(f, rows), :] = converted(a, f * per + e)

    def send_down(first, end):
        for h in range(first, end):
            last = nf if h == parts - 1 else 0
            each(1, nf, lambda k: down_copy(h, target(last - k if last else k), f).start())

    with jax.named_scope('send0'):
        send_weights(0)

    with jax.named_scope('send1'):
        send_weights(1)
    with jax.named_scope('send2'):
        send_weights(2)
    outer = (g == 0) | (g == GROUPS - 1)
    pl.when(jnp.logical_not(outer))(lambda: send_down(0, parts))

    with jax.named_scope('arrive'):
        settle(xs.at[0:GROUPS - 1], xsem.at[1])
        settle(vs.at[0:GROUPS - 1], vsem.at[1])

    def relay(k):
        token_relay(mate(k), m).start()
        share_relay(mate(k), m).start()
    each(1, width, relay)

    with jax.named_scope('relayed'):
        settle(xr.at[t, :, 0:width - 1], msem.at[1])
        settle(vr.at[:, 0:width - 1], nsem.at[1])
    each(1, nt, lambda k: gather_copy(other(k), t).start())

    lane = lax.broadcasted_iota(I32, (share, n_tok), 1) - lax.broadcasted_iota(I32, (share, n_tok), 0)

    def shares(n):
        i, w = n // width, lax.rem(n, width)
        eye = lane == lax.rem(i, split) * share
        for e in range(per):
            line = vr[i // split, w, pl.ds(m * per + e, 1), :]
            column = jnp.sum(jnp.where(eye, line, 0.0), axis=1, keepdims=True)
            wc[e, span(n, share), :] = jnp.broadcast_to(column, (share, LANES))
    each(0, nt * width, shares)

    with jax.named_scope('gather'):
        settle(xr.at[0:nt - 1], gsem.at[1])

    def product(a, e, i):
        total = jnp.zeros((plane, hidden), F32)
        for o in range(nt):
            left = xr[o, i].reshape(plane, cols)
            total += matmul(left, served[a][e, o * cols:(o + 1) * cols, :])
        return total * d_model ** (-0.5)

    with jax.named_scope('wait_gate'):
        settle(ws.at[0, 0:experts - per], wrecv.at[0])
    with jax.named_scope('wait_up'):
        settle(ws.at[1, 0:experts - per], wrecv.at[1])

    def activate(i):
        for e in range(per):
            v = product(0, e, i)
            value = v / (1.0 + jnp.exp(-v)) * product(1, e, i)
            value = value * wc[e, span(i, plane), 0:1]
            hs[span(i, plane), e * hidden:(e + 1) * hidden] = value.astype(BF16)
    pl.when(outer)(lambda: send_down(0, parts))
    with jax.named_scope('activate'):
        each(0, nt, activate)

    hidden_scale = (hidden * nt) ** (-0.5)
    blocks = pieces // parts
    quarter = pieces // GROUPS
    wide_blocks = blocks // GROUPS
    low = g < GROUPS // 2

    def piece_at(n):
        i, r = n // quarter, lax.rem(n, quarter)
        far = jnp.where(low, GROUPS + 1 - i, i - 2)
        z = jnp.where(i < 2, g ^ i, far)
        return (z * wide_blocks + lax.rem(r, wide_blocks)) * parts + r // wide_blocks

    def multiply(n):
        c = piece_at(n)
        h = lax.rem(c, parts)
        for q in range(joint):
            s = c // parts * joint + q

            @pl.when(s != f)
            def _():
                with jax.named_scope('wait_piece'):
                    down_copy(h, f, s).wait_recv()
        value = jnp.zeros((nt * plane, LANES), F32)
        for e in range(per):
            value += matmul(
                hs[:, e * hidden:(e + 1) * hidden], down_out[e, span(c, LANES), :], ((1,), (1,)))
        ps[c] = (value * hidden_scale).astype(BF16).reshape(2, nt // 2, plane, LANES)
        partial_copy(c, t + 1).start()

    def reduce(n):
        c = piece_at(n)
        with jax.named_scope('wait_partial'):
            partial_copy(c, t).wait_recv()
        total = ps[c, lax.rem(t, 2)].astype(F32) + pr[c].astype(F32)
        qs[c] = total.astype(BF16).reshape(crews, share, LANES)
        each(1, crews, lambda k: crew_copy(c, crew(k), crew(0)).start())

    def give_back(n):
        c = piece_at(n)
        with jax.named_scope('wait_mate'):
            settle(qs.at[c, 0:crews - 1], qrecv.at[c])
        total = qs[c, crew(0)].astype(F32)
        for k in range(1, crews):
            total += qr[crew(k), c].astype(F32)
        rs[c] = total.astype(BF16)
        owner = c // per_owner
        local = (home == g) & (owner == t)

        @pl.when(local)
        def _():
            ret[lax.rem(c, per_owner), span(g * split + rest, share), :] = rs[c]

        @pl.when(jnp.logical_not(local))
        def _():
            return_copy(c, home * width + m, owner, g * split + rest).start()

    def step(n):
        @pl.when(n < pieces)
        def _():
            multiply(n)

        @pl.when((n >= PAIR_LAG) & (n < pieces + PAIR_LAG))
        def _():
            reduce(n - PAIR_LAG)

        @pl.when(n >= CREW_LAG)
        def _():
            give_back(n - CREW_LAG)
    each(0, pieces + CREW_LAG, step)

    own_share = pieces - per_owner

    @pl.when(home == g)
    def _():
        settle(ret.at[:, 0:GROUPS * slots - share], rsem.at[1])
        settle(rs.at[0:own_share], rsem.at[0])

    @pl.when(home != g)
    def _():
        settle(ret, rsem.at[1])
        settle(rs, rsem.at[0])

    for a in range(3):
        settle(ws.at[a, 0:experts - per], wsend.at[a])
    settle(xs.at[0:GROUPS - 1], xsem.at[0])
    settle(vs.at[0:GROUPS - 1], vsem.at[0])
    settle(xr.at[t, :, 0:width - 1], msem.at[0])
    settle(vr.at[:, 0:width - 1], nsem.at[0])
    settle(xr.at[0:nt - 1], gsem.at[0])
    settle(pr, psend)
    settle(qs.at[:, 0:crews - 1], qsend)


def finish_kernel(
    ids_t, ret, gate, up, down, gate_out, up_out, down_out, combined, result, sem, *, per_group
):
    outs = [
        pltpu.make_async_copy(source, target, sem.at[a])
        for a, (source, target) in enumerate(((gate, gate_out), (up, up_out), (down, down_out)))
    ]
    for copy in outs:
        copy.start()
    chunks, slots, width = ret.shape
    chosen = placement(ids_t, per_group, slots // GROUPS)
    for i in range(chunks):
        value = matmul(chosen, ret[i], ((0,), (0,)))
        result[:, i * width:(i + 1) * width] = value.astype(BF16)
    last = pltpu.make_async_copy(result, combined, sem.at[3])
    last.start()
    for copy in outs:
        copy.wait()
    last.wait()


def body(nf, nt, tokens, route_ids, route_weights, norm_gain, gate_weight, up_weight, down_weight):
    experts, rows, hidden = gate_weight.shape
    n_tok, d_model = tokens.shape
    per = experts // nf
    cols = d_model // nt
    slots = n_tok // route_ids.shape[1]
    width = nf // GROUPS
    per_group = experts // GROUPS
    lines = max(8, per_group)
    crews = nt // 2 * width
    split = nt // GROUPS
    share = slots // split
    parts = max(1, rows // LANES)
    pieces = d_model // LANES
    per_owner = cols // LANES
    shape = (per, nf * rows, hidden)
    vmem, anywhere = pl.BlockSpec(memory_space=pltpu.VMEM), pl.BlockSpec(memory_space=pl.ANY)
    dma = pltpu.SemaphoreType.DMA
    ids_t, weights_t = route_ids.T, route_weights.T
    *served, ret = pl.pallas_call(
        functools.partial(kernel, nf, nt),
        out_shape=[pltpu.VMEM(shape, BF16)] * 3
        + [pltpu.VMEM((per_owner, GROUPS * slots, LANES), BF16)],
        in_specs=[anywhere] * 7,
        out_specs=[vmem] * 4,
        scratch_shapes=[
            pltpu.VMEM((n_tok, d_model), BF16),
            pltpu.VMEM(ids_t.shape, I32),
            pltpu.VMEM(weights_t.shape, F32),
            pltpu.VMEM((1, rows), F32),
            pltpu.VMEM((2, experts, rows, hidden), F32),
            pltpu.VMEM((3, experts, rows, hidden), BF16),
            pltpu.VMEM((GROUPS, split, share, cols), BF16),
            pltpu.VMEM((GROUPS, lines, n_tok), F32),
            pltpu.VMEM((nt, nt, width, share, cols), BF16),
            pltpu.VMEM((GROUPS, width, lines, n_tok), F32),
            pltpu.VMEM((per, nf * slots, LANES), F32),
            pltpu.VMEM((nf * slots, per * hidden), BF16),
            pltpu.VMEM((pieces, 2, nt // 2, width * share, LANES), BF16),
            pltpu.VMEM((pieces, nt // 2, width * share, LANES), BF16),
            pltpu.VMEM((pieces, crews, share, LANES), BF16),
            pltpu.VMEM((crews, pieces, share, LANES), BF16),
            pltpu.VMEM((pieces, share, LANES), BF16),
            dma((4,)), dma((nf,)), dma((3,)), dma((2,)), dma((parts, nf)),
            dma((2,)), dma((2,)), dma((2,)), dma((2,)), dma((2,)),
            dma, dma((pieces,)), dma, dma((pieces,)), dma((2,)),
        ],
        compiler_params=pltpu.CompilerParams(
            collective_id=0, has_side_effects=True, vmem_limit_bytes=54 * 1024 * 1024
        ),
    )(tokens, ids_t, weights_t, norm_gain[None, :], gate_weight, up_weight, down_weight)
    out = jax.ShapeDtypeStruct(shape, BF16)
    return pl.pallas_call(
        functools.partial(finish_kernel, per_group=per_group),
        out_shape=(out, out, out, jax.ShapeDtypeStruct((n_tok, cols), BF16)),
        in_specs=[vmem] * 5,
        out_specs=(anywhere,) * 4,
        scratch_shapes=[pltpu.VMEM((n_tok, cols), BF16), dma((4,))],
        compiler_params=pltpu.CompilerParams(vmem_limit_bytes=16 * 1024 * 1024),
    )(ids_t, ret, *served)


def solution(mesh):
    split = P(None, "fs", "tp")
    served = P("fs", None, "tp")
    return jax.shard_map(
        functools.partial(body, mesh.shape["fs"], mesh.shape["tp"]),
        mesh=mesh,
        in_specs=(P("fs", None), P("fs", None), P("fs", None), P("fs"), split, split, split),
        out_specs=(served, served, served, P("fs", "tp")),
        check_vma=False,
    )
```

```python
import functools

import jax
import jax.numpy as jnp
from jax import lax
from jax.experimental import pallas as pl
from jax.experimental.pallas import tpu as pltpu
from jax.sharding import PartitionSpec as P

GROUPS = 4
ORDER = ((('near', 'inner', 'outer'), ('inner', 'outer', 'near')), (('near', 'inner', 'outer'), ('inner', 'outer', 'near')), (('near', 'inner', 'outer'), ('inner', 'outer', 'near')), (('near', 'outer', 'inner'), ('near', 'outer', 'inner')))
EPSILON = 1e-06
MESH = pl.DeviceIdType.MESH
PAIR_LAG, CREW_LAG = 1, 3
LANES = 128
F32, BF16, I32 = jnp.float32, jnp.bfloat16, jnp.int32


def matmul(a, b, contract=((1,), (0,))):
    return lax.dot_general(a, b, (contract, ((), ())), preferred_element_type=F32)


def placement(ids_t, per_group, slots):
    n_tok = ids_t.shape[1]
    slot = lax.broadcasted_iota(I32, (GROUPS * slots, n_tok), 0)
    member = ids_t[0:1, :] // per_group == slot // slots
    earlier = (
        lax.broadcasted_iota(I32, (n_tok, n_tok), 0) < lax.broadcasted_iota(I32, (n_tok, n_tok), 1)
    )
    place = matmul(member.astype(F32).astype(BF16), earlier.astype(F32).astype(BF16))
    return (member & (place.astype(I32) == slot % slots)).astype(F32).astype(BF16)


def each(first, last, action):
    def go(k, carry):
        action(k)
        return carry
    lax.fori_loop(first, last, go, 0)


def kernel(
    nf, nt,
    tokens_in, ids_in, weights_in, gain_in, gate, up, down,
    gate_out, up_out, down_out, ret,
    tokens, ids_t, weights_t, gain,
    wf, ws, xs, vs, xr, vr, wc, hs, ps, pr, qs, qr, rs,
    in_sem, load_sem, wsend, wrecv, drecv, xsem, vsem, msem, nsem, gsem, psend, precv, qsend, qrecv, rsem,
):
    f, t = lax.axis_index("fs"), lax.axis_index("tp")
    experts, rows, hidden = gate.shape
    n_tok, d_model = tokens.shape
    per = experts // nf
    cols = d_model // nt
    width = nf // GROUPS
    slots = n_tok // ids_t.shape[0]
    split = nt // GROUPS
    share = slots // split
    per_group = experts // GROUPS
    plane = width * share
    parts = max(1, rows // LANES)
    part = rows // parts
    joint = max(1, LANES // rows)
    pieces = d_model // LANES
    per_owner = cols // LANES
    g, m = f // width, lax.rem(f, width)
    shift = t // 2 + nt // 2 * lax.rem(t, 2)
    home, rest = shift // split, lax.rem(shift, split)
    crews = nt // 2 * width
    served = (gate_out, up_out, down_out)

    lower = g < GROUPS // 2
    outer = (g == 0) | (g == GROUPS - 1)
    planes = {
        "near": g ^ 1,
        "inner": jnp.where(lower, GROUPS // 2, GROUPS // 2 - 1),
        "outer": jnp.where(lower, GROUPS - 1, 0),
    }

    def pick(order, j):
        first, second, third = (planes[name] for name in order)
        return jnp.where(j == 0, first, jnp.where(j == 1, second, third))

    def target(turn, k):
        from_outer, from_inner = ORDER[turn]
        j, r = k // width - 1, lax.rem(k, width)
        z = jnp.where(outer, pick(from_outer, j), pick(from_inner, j))
        x = lax.rem(m + r + 1, width) if turn == 3 else jnp.where(lower, r, width - 1 - r)
        return jnp.where(k < width, g * width + lax.rem(m + k, width), z * width + x)

    def other(k):
        return lax.rem(t + k, nt)

    def mate(k):
        return lax.rem(m + k, width)

    def group(k):
        return lax.rem(g + k, GROUPS)

    def span(start, size):
        return pl.ds(pl.multiple_of(start * size, size), size)

    def loads(a, k):
        p = jnp.where(k == 0, f, target(a, k))
        return pltpu.make_async_copy(
            (gate, up, down)[a].at[pl.ds(p * per, per)],
            wf.at[a % 2, pl.ds(p * per, per)],
            load_sem.at[k],
        )

    def remote(src, dst, send, recv, device):
        return pltpu.make_async_remote_copy(
            src_ref=src, dst_ref=dst, send_sem=send, recv_sem=recv,
            device_id=device, device_id_type=MESH,
        )

    def settle(ref, sem):
        pltpu.make_async_copy(ref, ref, sem).wait()

    def weight_copy(a, p, src):
        return remote(
            ws.at[a, pl.ds(p * per, per)],
            served[a].at[:, span(src, rows), :],
            wsend.at[a], wrecv.at[a], {"fs": p},
        )

    def down_copy(h, p, src):
        return remote(
            ws.at[2, pl.ds(p * per, per), span(h, part), :],
            down_out.at[:, span(src * parts + h, part), :],
            wsend.at[2], drecv.at[h, src], {"fs": p},
        )

    def token_copy(to, src):
        return remote(
            xs.at[to], xr.at[t, pl.ds(src * split, split), m], xsem.at[0], xsem.at[1], {"fs": to * width + m}
        )

    def share_copy(to, src):
        return remote(vs.at[to], vr.at[src, m], vsem.at[0], vsem.at[1], {"fs": to * width + m})

    def token_relay(to, src):
        return remote(
            xr.at[t, :, src], xr.at[t, :, src], msem.at[0], msem.at[1], {"fs": g * width + to}
        )

    def share_relay(to, src):
        return remote(
            vr.at[:, src], vr.at[:, src], nsem.at[0], nsem.at[1], {"fs": g * width + to}
        )

    def gather_copy(to, src):
        return remote(xr.at[src], xr.at[src], gsem.at[0], gsem.at[1], {"tp": to})

    def partial_copy(c, to):
        return remote(
            ps.at[c, lax.rem(to, 2)], pr.at[c], psend, precv.at[c], {"tp": t // 2 * 2 + lax.rem(to, 2)}
        )

    def crew(k):
        return lax.rem(t // 2 * width + m + k, crews)

    def crew_copy(c, to, src):
        return remote(
            qs.at[c, to], qr.at[src, c], qsend, qrecv.at[c],
            {"fs": g * width + lax.rem(to, width), "tp": to // width * 2 + lax.rem(t, 2)},
        )

    def return_copy(c, to_fs, to_tp, src):
        i = lax.rem(c, per_owner)
        return remote(
            rs.at[c], ret.at[i, span(src, share), :],
            rsem.at[0], rsem.at[1], {"fs": to_fs, "tp": to_tp},
        )

    barrier = pltpu.get_barrier_semaphore()
    each(1, nf, lambda k: pl.semaphore_signal(
        barrier, inc=1, device_id={"fs": lax.rem(f + k, nf)}, device_id_type=MESH))
    each(1, nt, lambda k: pl.semaphore_signal(
        barrier, inc=1, device_id={"tp": other(k)}, device_id_type=MESH))
    inputs = [
        pltpu.make_async_copy(src, dst, in_sem.at[i])
        for i, (src, dst) in enumerate((
            (tokens_in, tokens), (ids_in, ids_t), (weights_in, weights_t), (gain_in, gain)))
    ]
    for copy in inputs:
        copy.start()
    each(1, nf, lambda k: loads(0, k).start())
    loads(0, 0).start()
    for copy in inputs:
        copy.wait()
    wide = tokens[...].astype(F32)
    scale = lax.rsqrt(jnp.mean(wide * wide, axis=1, keepdims=True) + EPSILON)
    own = tokens[:, span(t, cols)].astype(F32)
    normed = (own * scale).astype(BF16)
    chosen = placement(ids_t, per_group, slots)
    xs[...] = matmul(chosen, normed).reshape(GROUPS, split, share, cols).astype(BF16)
    vs[...] = jnp.zeros(vs.shape, F32)
    row = lax.broadcasted_iota(I32, (vs.shape[1], n_tok), 0)
    for i in range(GROUPS):
        value = jnp.zeros((vs.shape[1], n_tok), F32)
        for r in range(ids_t.shape[0]):
            value += jnp.where(
                (row < per_group) & (row + i * per_group == ids_t[r:r + 1, :]),
                weights_t[r:r + 1, :], 0.0)
        high = value.astype(BF16)
        low = (value - high.astype(F32)).astype(BF16)
        here = chosen[i * slots:(i + 1) * slots]
        vs[i, :, 0:slots] = (
            matmul(high, here, ((1,), (1,))) + matmul(low, here, ((1,), (1,))))

    with jax.named_scope('barrier'):
        pl.semaphore_wait(barrier, nf + nt - 2)

    def dispatch(k):
        token_copy(group(k), g).start()
        share_copy(group(k), g).start()
    each(1, GROUPS, dispatch)
    for q in range(split):
        xr[t, g * split + q, m] = xs[g, q]
    vr[g, m] = vs[g]

    square = lax.broadcasted_iota(I32, (rows, rows), 0) == lax.broadcasted_iota(I32, (rows, rows), 1)
    gain_column = jnp.sum(jnp.where(square, gain[...], 0.0), axis=1, keepdims=True)

    def converted(a, n):
        value = wf[a % 2, n]
        if a < 2:
            value = value * gain_column
        return value.astype(BF16)

    def send_weights(a):
        def load_next(k):
            if a < 2:
                loads(a + 1, k).start()

        def one(k):
            p = target(a, k)
            loads(a, k).wait()
            load_next(k)
            for e in range(per):
                ws[a, p * per + e] = converted(a, p * per + e)
            if a < 2:
                weight_copy(a, p, f).start()
        each(1, nf, one)
        loads(a, 0).wait()
        load_next(0)
        for e in range(per):
            served[a][e, span(f, rows), :] = converted(a, f * per + e)

    def send_down(first, end):
        for h in range(first, end):
            each(1, nf, lambda k: down_copy(h, target(2 + (h > 0), k), f).start())

    with jax.named_scope('send0'):
        send_weights(0)

    with jax.named_scope('send1'):
        send_weights(1)
    with jax.named_scope('send2'):
        send_weights(2)
    pl.when(jnp.logical_not(outer))(lambda: send_down(0, parts))

    with jax.named_scope('arrive'):
        settle(xs.at[0:GROUPS - 1], xsem.at[1])
        settle(vs.at[0:GROUPS - 1], vsem.at[1])

    def relay(k):
        token_relay(mate(k), m).start()
        share_relay(mate(k), m).start()
    each(1, width, relay)

    with jax.named_scope('relayed'):
        settle(xr.at[t, :, 0:width - 1], msem.at[1])
        settle(vr.at[:, 0:width - 1], nsem.at[1])
    each(1, nt, lambda k: gather_copy(other(k), t).start())

    lane = lax.broadcasted_iota(I32, (share, n_tok), 1) - lax.broadcasted_iota(I32, (share, n_tok), 0)

    def shares(n):
        i, w = n // width, lax.rem(n, width)
        eye = lane == lax.rem(i, split) * share
        for e in range(per):
            line = vr[i // split, w, pl.ds(m * per + e, 1), :]
            column = jnp.sum(jnp.where(eye, line, 0.0), axis=1, keepdims=True)
            wc[e, span(n, share), :] = jnp.broadcast_to(column, (share, LANES))
    each(0, nt * width, shares)

    with jax.named_scope('gather'):
        settle(xr.at[0:nt - 1], gsem.at[1])

    def product(a, e, i):
        total = jnp.zeros((plane, hidden), F32)
        for o in range(nt):
            left = xr[o, i].reshape(plane, cols)
            total += matmul(left, served[a][e, o * cols:(o + 1) * cols, :])
        return total * d_model ** (-0.5)

    with jax.named_scope('wait_gate'):
        settle(ws.at[0, 0:experts - per], wrecv.at[0])
    with jax.named_scope('wait_up'):
        settle(ws.at[1, 0:experts - per], wrecv.at[1])

    def activate(i):
        for e in range(per):
            v = product(0, e, i)
            value = v / (1.0 + jnp.exp(-v)) * product(1, e, i)
            value = value * wc[e, span(i, plane), 0:1]
            hs[span(i, plane), e * hidden:(e + 1) * hidden] = value.astype(BF16)
    pl.when(outer)(lambda: send_down(0, parts))
    with jax.named_scope('activate'):
        each(0, nt, activate)

    hidden_scale = (hidden * nt) ** (-0.5)
    blocks = pieces // parts
    quarter = pieces // GROUPS
    wide_blocks = blocks // GROUPS
    def piece_at(n):
        j, r = (n - quarter) // wide_blocks, lax.rem(n, wide_blocks)
        first = n < quarter
        h = jnp.where(first, n // wide_blocks, jnp.where(outer, lax.rem(j, parts), j // 3))
        turn = jnp.where(outer, j // parts, lax.rem(j, 3))
        turn = jnp.where((turn < 2) & (h > 0) & jnp.logical_not(outer), 1 - turn, turn)
        far = jnp.where(lower, GROUPS - turn, turn - 1)
        z = jnp.where(first, g, jnp.where(turn == 0, g ^ 1, far))
        return (z * wide_blocks + r) * parts + h

    def multiply(n):
        c = piece_at(n)
        h = lax.rem(c, parts)
        for q in range(joint):
            s = c // parts * joint + q

            @pl.when(s != f)
            def _():
                with jax.named_scope('wait_piece'):
                    down_copy(h, f, s).wait_recv()
        value = jnp.zeros((nt * plane, LANES), F32)
        for e in range(per):
            value += matmul(
                hs[:, e * hidden:(e + 1) * hidden], down_out[e, span(c, LANES), :], ((1,), (1,)))
        ps[c] = (value * hidden_scale).astype(BF16).reshape(2, nt // 2, plane, LANES)
        partial_copy(c, t + 1).start()

    def reduce(n):
        c = piece_at(n)
        with jax.named_scope('wait_partial'):
            partial_copy(c, t).wait_recv()
        total = ps[c, lax.rem(t, 2)].astype(F32) + pr[c].astype(F32)
        qs[c] = total.astype(BF16).reshape(crews, share, LANES)
        each(1, crews, lambda k: crew_copy(c, crew(k), crew(0)).start())

    def give_back(n):
        c = piece_at(n)
        with jax.named_scope('wait_mate'):
            settle(qs.at[c, 0:crews - 1], qrecv.at[c])
        total = qs[c, crew(0)].astype(F32)
        for k in range(1, crews):
            total += qr[crew(k), c].astype(F32)
        rs[c] = total.astype(BF16)
        owner = c // per_owner
        local = (home == g) & (owner == t)

        @pl.when(local)
        def _():
            ret[lax.rem(c, per_owner), span(g * split + rest, share), :] = rs[c]

        pl.when(jnp.logical_not(crossing) | (n >= late) | (n < 0))(lambda: send_back(n))

    crossing = outer & ((home < GROUPS // 2) != (g < GROUPS // 2))

    def send_back(n):
        c = piece_at(n)
        owner = c // per_owner

        @pl.when((home != g) | (owner != t))
        def _():
            return_copy(c, home * width + m, owner, g * split + rest).start()

    late = pieces - wide_blocks

    def step(n):
        multiply(n)
        pl.when(n >= PAIR_LAG)(lambda: reduce(n - PAIR_LAG))
        pl.when(n >= CREW_LAG)(lambda: give_back(n - CREW_LAG))
    each(0, late, step)
    each(late - PAIR_LAG, late, reduce)
    each(late - CREW_LAG, late, give_back)
    each(late, pieces, multiply)
    each(late, pieces, reduce)
    each(late, pieces, give_back)
    pl.when(crossing)(lambda: each(0, late, send_back))

    own_share = pieces - per_owner

    @pl.when(home == g)
    def _():
        settle(ret.at[:, 0:GROUPS * slots - share], rsem.at[1])
        settle(rs.at[0:own_share], rsem.at[0])

    @pl.when(home != g)
    def _():
        settle(ret, rsem.at[1])
        settle(rs, rsem.at[0])

    for a in range(3):
        settle(ws.at[a, 0:experts - per], wsend.at[a])
    settle(xs.at[0:GROUPS - 1], xsem.at[0])
    settle(vs.at[0:GROUPS - 1], vsem.at[0])
    settle(xr.at[t, :, 0:width - 1], msem.at[0])
    settle(vr.at[:, 0:width - 1], nsem.at[0])
    settle(xr.at[0:nt - 1], gsem.at[0])
    settle(pr, psend)
    settle(qs.at[:, 0:crews - 1], qsend)


def finish_kernel(
    ids_t, ret, gate, up, down, gate_out, up_out, down_out, combined, result, sem, *, per_group
):
    outs = [
        pltpu.make_async_copy(source, target, sem.at[a])
        for a, (source, target) in enumerate(((gate, gate_out), (up, up_out), (down, down_out)))
    ]
    for copy in outs:
        copy.start()
    chunks, slots, width = ret.shape
    chosen = placement(ids_t, per_group, slots // GROUPS)
    for i in range(chunks):
        value = matmul(chosen, ret[i], ((0,), (0,)))
        result[:, i * width:(i + 1) * width] = value.astype(BF16)
    last = pltpu.make_async_copy(result, combined, sem.at[3])
    last.start()
    for copy in outs:
        copy.wait()
    last.wait()


def body(nf, nt, tokens, route_ids, route_weights, norm_gain, gate_weight, up_weight, down_weight):
    experts, rows, hidden = gate_weight.shape
    n_tok, d_model = tokens.shape
    per = experts // nf
    cols = d_model // nt
    slots = n_tok // route_ids.shape[1]
    width = nf // GROUPS
    per_group = experts // GROUPS
    lines = max(8, per_group)
    crews = nt // 2 * width
    split = nt // GROUPS
    share = slots // split
    parts = max(1, rows // LANES)
    pieces = d_model // LANES
    per_owner = cols // LANES
    shape = (per, nf * rows, hidden)
    vmem, anywhere = pl.BlockSpec(memory_space=pltpu.VMEM), pl.BlockSpec(memory_space=pl.ANY)
    dma = pltpu.SemaphoreType.DMA
    ids_t, weights_t = route_ids.T, route_weights.T
    *served, ret = pl.pallas_call(
        functools.partial(kernel, nf, nt),
        out_shape=[pltpu.VMEM(shape, BF16)] * 3
        + [pltpu.VMEM((per_owner, GROUPS * slots, LANES), BF16)],
        in_specs=[anywhere] * 7,
        out_specs=[vmem] * 4,
        scratch_shapes=[
            pltpu.VMEM((n_tok, d_model), BF16),
            pltpu.VMEM(ids_t.shape, I32),
            pltpu.VMEM(weights_t.shape, F32),
            pltpu.VMEM((1, rows), F32),
            pltpu.VMEM((2, experts, rows, hidden), F32),
            pltpu.VMEM((3, experts, rows, hidden), BF16),
            pltpu.VMEM((GROUPS, split, share, cols), BF16),
            pltpu.VMEM((GROUPS, lines, n_tok), F32),
            pltpu.VMEM((nt, nt, width, share, cols), BF16),
            pltpu.VMEM((GROUPS, width, lines, n_tok), F32),
            pltpu.VMEM((per, nf * slots, LANES), F32),
            pltpu.VMEM((nf * slots, per * hidden), BF16),
            pltpu.VMEM((pieces, 2, nt // 2, width * share, LANES), BF16),
            pltpu.VMEM((pieces, nt // 2, width * share, LANES), BF16),
            pltpu.VMEM((pieces, crews, share, LANES), BF16),
            pltpu.VMEM((crews, pieces, share, LANES), BF16),
            pltpu.VMEM((pieces, share, LANES), BF16),
            dma((4,)), dma((nf,)), dma((3,)), dma((2,)), dma((parts, nf)),
            dma((2,)), dma((2,)), dma((2,)), dma((2,)), dma((2,)),
            dma, dma((pieces,)), dma, dma((pieces,)), dma((2,)),
        ],
        compiler_params=pltpu.CompilerParams(
            collective_id=0, has_side_effects=True, vmem_limit_bytes=54 * 1024 * 1024
        ),
    )(tokens, ids_t, weights_t, norm_gain[None, :], gate_weight, up_weight, down_weight)
    out = jax.ShapeDtypeStruct(shape, BF16)
    return pl.pallas_call(
        functools.partial(finish_kernel, per_group=per_group),
        out_shape=(out, out, out, jax.ShapeDtypeStruct((n_tok, cols), BF16)),
        in_specs=[vmem] * 5,
        out_specs=(anywhere,) * 4,
        scratch_shapes=[pltpu.VMEM((n_tok, cols), BF16), dma((4,))],
        compiler_params=pltpu.CompilerParams(vmem_limit_bytes=16 * 1024 * 1024),
    )(ids_t, ret, *served)


def solution(mesh):
    split = P(None, "fs", "tp")
    served = P("fs", None, "tp")
    return jax.shard_map(
        functools.partial(body, mesh.shape["fs"], mesh.shape["tp"]),
        mesh=mesh,
        in_specs=(P("fs", None), P("fs", None), P("fs", None), P("fs"), split, split, split),
        out_specs=(served, served, served, P("fs", "tp")),
        check_vma=False,
    )
```

```python
import functools

import jax
import jax.numpy as jnp
from jax import lax
from jax.experimental import pallas as pl
from jax.experimental.pallas import tpu as pltpu
from jax.sharding import PartitionSpec as P

GROUPS = 4
ORDER = ((('near', 'inner', 'outer'), ('inner', 'outer', 'near')), (('near', 'inner', 'outer'), ('inner', 'outer', 'near')), (('near', 'inner', 'outer'), ('inner', 'outer', 'near')), (('near', 'outer', 'inner'), ('near', 'outer', 'inner')))
EPSILON = 1e-06
MESH = pl.DeviceIdType.MESH
PAIR_LAG, CREW_LAG = 1, 3
LANES = 128
F32, BF16, I32 = jnp.float32, jnp.bfloat16, jnp.int32


def matmul(a, b, contract=((1,), (0,))):
    return lax.dot_general(a, b, (contract, ((), ())), preferred_element_type=F32)


def placement(ids_t, per_group, slots):
    n_tok = ids_t.shape[1]
    slot = lax.broadcasted_iota(I32, (GROUPS * slots, n_tok), 0)
    member = ids_t[0:1, :] // per_group == slot // slots
    earlier = (
        lax.broadcasted_iota(I32, (n_tok, n_tok), 0) < lax.broadcasted_iota(I32, (n_tok, n_tok), 1)
    )
    place = matmul(member.astype(F32).astype(BF16), earlier.astype(F32).astype(BF16))
    return (member & (place.astype(I32) == slot % slots)).astype(F32).astype(BF16)


def each(first, last, action):
    def go(k, carry):
        action(k)
        return carry
    lax.fori_loop(first, last, go, 0)


def kernel(
    nf, nt,
    tokens_in, ids_in, weights_in, gain_in, gate, up, down,
    gate_out, up_out, down_out, ret,
    tokens, ids_t, weights_t, gain,
    wf, ws, xs, vs, xr, vr, wc, hs, ps, pr, qs, qr, rs,
    in_sem, load_sem, wsend, wrecv, drecv, xsem, vsem, msem, nsem, gsem, psend, precv, qsend, qrecv, rsem,
):
    f, t = lax.axis_index("fs"), lax.axis_index("tp")
    experts, rows, hidden = gate.shape
    n_tok, d_model = tokens.shape
    per = experts // nf
    cols = d_model // nt
    width = nf // GROUPS
    slots = n_tok // ids_t.shape[0]
    split = nt // GROUPS
    share = slots // split
    per_group = experts // GROUPS
    plane = width * share
    parts = max(1, rows // LANES)
    part = rows // parts
    joint = max(1, LANES // rows)
    pieces = d_model // LANES
    per_owner = cols // LANES
    g, m = f // width, lax.rem(f, width)
    shift = t // 2 + nt // 2 * lax.rem(t, 2)
    home, rest = shift // split, lax.rem(shift, split)
    crews = nt // 2 * width
    served = (gate_out, up_out, down_out)

    lower = g < GROUPS // 2
    outer = (g == 0) | (g == GROUPS - 1)
    planes = {
        "near": g ^ 1,
        "inner": jnp.where(lower, GROUPS // 2, GROUPS // 2 - 1),
        "outer": jnp.where(lower, GROUPS - 1, 0),
    }

    def pick(order, j):
        first, second, third = (planes[name] for name in order)
        return jnp.where(j == 0, first, jnp.where(j == 1, second, third))

    def target(turn, k):
        from_outer, from_inner = ORDER[turn]
        j, r = k // width - 1, lax.rem(k, width)
        z = jnp.where(outer, pick(from_outer, j), pick(from_inner, j))
        x = lax.rem(m + r + 1, width) if turn == 3 else jnp.where(lower, r, width - 1 - r)
        return jnp.where(k < width, g * width + lax.rem(m + k, width), z * width + x)

    def other(k):
        return lax.rem(t + k, nt)

    def mate(k):
        return lax.rem(m + k, width)

    def group(k):
        return lax.rem(g + k, GROUPS)

    def span(start, size):
        return pl.ds(pl.multiple_of(start * size, size), size)

    def loads(a, k):
        p = jnp.where(k == 0, f, target(a, k))
        return pltpu.make_async_copy(
            (gate, up, down)[a].at[pl.ds(p * per, per)],
            wf.at[a % 2, pl.ds(p * per, per)],
            load_sem.at[k],
        )

    def remote(src, dst, send, recv, device):
        return pltpu.make_async_remote_copy(
            src_ref=src, dst_ref=dst, send_sem=send, recv_sem=recv,
            device_id=device, device_id_type=MESH,
        )

    def settle(ref, sem):
        pltpu.make_async_copy(ref, ref, sem).wait()

    def weight_copy(a, p, src):
        return remote(
            ws.at[a, pl.ds(p * per, per)],
            served[a].at[:, span(src, rows), :],
            wsend.at[a], wrecv.at[a], {"fs": p},
        )

    def down_copy(h, p, src):
        return remote(
            ws.at[2, pl.ds(p * per, per), span(h, part), :],
            down_out.at[:, span(src * parts + h, part), :],
            wsend.at[2], drecv.at[h, src], {"fs": p},
        )

    def token_copy(to, src):
        return remote(
            xs.at[to], xr.at[t, pl.ds(src * split, split), m], xsem.at[0], xsem.at[1], {"fs": to * width + m}
        )

    def share_copy(to, src):
        return remote(vs.at[to], vr.at[src, m], vsem.at[0], vsem.at[1], {"fs": to * width + m})

    def token_relay(to, src):
        return remote(
            xr.at[t, :, src], xr.at[t, :, src], msem.at[0], msem.at[1], {"fs": g * width + to}
        )

    def share_relay(to, src):
        return remote(
            vr.at[:, src], vr.at[:, src], nsem.at[0], nsem.at[1], {"fs": g * width + to}
        )

    def gather_copy(to, src):
        return remote(xr.at[src], xr.at[src], gsem.at[0], gsem.at[1], {"tp": to})

    def partial_copy(c, to):
        return remote(
            ps.at[c, lax.rem(to, 2)], pr.at[c], psend, precv.at[c], {"tp": t // 2 * 2 + lax.rem(to, 2)}
        )

    def crew(k):
        return lax.rem(t // 2 * width + m + k, crews)

    def crew_copy(c, to, src):
        return remote(
            qs.at[c, to], qr.at[src, c], qsend, qrecv.at[c],
            {"fs": g * width + lax.rem(to, width), "tp": to // width * 2 + lax.rem(t, 2)},
        )

    def return_copy(c, to_fs, to_tp, src):
        i = lax.rem(c, per_owner)
        return remote(
            rs.at[c], ret.at[i, span(src, share), :],
            rsem.at[0], rsem.at[1], {"fs": to_fs, "tp": to_tp},
        )

    barrier = pltpu.get_barrier_semaphore()
    each(1, nf, lambda k: pl.semaphore_signal(
        barrier, inc=1, device_id={"fs": lax.rem(f + k, nf)}, device_id_type=MESH))
    each(1, nt, lambda k: pl.semaphore_signal(
        barrier, inc=1, device_id={"tp": other(k)}, device_id_type=MESH))
    inputs = [
        pltpu.make_async_copy(src, dst, in_sem.at[i])
        for i, (src, dst) in enumerate((
            (tokens_in, tokens), (ids_in, ids_t), (weights_in, weights_t), (gain_in, gain)))
    ]
    for copy in inputs:
        copy.start()
    each(1, nf, lambda k: loads(0, k).start())
    loads(0, 0).start()
    for copy in inputs:
        copy.wait()
    wide = tokens[...].astype(F32)
    scale = lax.rsqrt(jnp.mean(wide * wide, axis=1, keepdims=True) + EPSILON)
    own = tokens[:, span(t, cols)].astype(F32)
    normed = (own * scale).astype(BF16)
    chosen = placement(ids_t, per_group, slots)
    xs[...] = matmul(chosen, normed).reshape(GROUPS, split, share, cols).astype(BF16)
    vs[...] = jnp.zeros(vs.shape, F32)
    row = lax.broadcasted_iota(I32, (vs.shape[1], n_tok), 0)
    for i in range(GROUPS):
        value = jnp.zeros((vs.shape[1], n_tok), F32)
        for r in range(ids_t.shape[0]):
            value += jnp.where(
                (row < per_group) & (row + i * per_group == ids_t[r:r + 1, :]),
                weights_t[r:r + 1, :], 0.0)
        high = value.astype(BF16)
        low = (value - high.astype(F32)).astype(BF16)
        here = chosen[i * slots:(i + 1) * slots]
        vs[i, :, 0:slots] = (
            matmul(high, here, ((1,), (1,))) + matmul(low, here, ((1,), (1,))))

    with jax.named_scope('barrier'):
        pl.semaphore_wait(barrier, nf + nt - 2)

    def dispatch(k):
        token_copy(group(k), g).start()
        share_copy(group(k), g).start()
    each(1, GROUPS, dispatch)
    for q in range(split):
        xr[t, g * split + q, m] = xs[g, q]
    vr[g, m] = vs[g]

    square = lax.broadcasted_iota(I32, (rows, rows), 0) == lax.broadcasted_iota(I32, (rows, rows), 1)
    gain_column = jnp.sum(jnp.where(square, gain[...], 0.0), axis=1, keepdims=True)

    def converted(a, n):
        value = wf[a % 2, n]
        if a < 2:
            value = value * gain_column
        return value.astype(BF16)

    def send_weights(a):
        def load_next(k):
            if a < 2:
                loads(a + 1, k).start()

        def one(k):
            p = target(a, k)
            loads(a, k).wait()
            load_next(k)
            for e in range(per):
                ws[a, p * per + e] = converted(a, p * per + e)
            if a < 2:
                weight_copy(a, p, f).start()
        each(1, nf, one)
        loads(a, 0).wait()
        load_next(0)
        for e in range(per):
            served[a][e, span(f, rows), :] = converted(a, f * per + e)

    def send_down(first, end):
        for h in range(first, end):
            each(1, nf, lambda k: down_copy(h, target(2 + (h > 0), k), f).start())

    with jax.named_scope('send0'):
        send_weights(0)

    with jax.named_scope('send1'):
        send_weights(1)
    with jax.named_scope('send2'):
        send_weights(2)
    pl.when(jnp.logical_not(outer))(lambda: send_down(0, parts))

    with jax.named_scope('arrive'):
        settle(xs.at[0:GROUPS - 1], xsem.at[1])
        settle(vs.at[0:GROUPS - 1], vsem.at[1])

    def relay(k):
        token_relay(mate(k), m).start()
        share_relay(mate(k), m).start()
    each(1, width, relay)

    with jax.named_scope('relayed'):
        settle(xr.at[t, :, 0:width - 1], msem.at[1])
        settle(vr.at[:, 0:width - 1], nsem.at[1])
    each(1, nt, lambda k: gather_copy(other(k), t).start())

    lane = lax.broadcasted_iota(I32, (share, n_tok), 1) - lax.broadcasted_iota(I32, (share, n_tok), 0)

    def shares(n):
        i, w = n // width, lax.rem(n, width)
        eye = lane == lax.rem(i, split) * share
        for e in range(per):
            line = vr[i // split, w, pl.ds(m * per + e, 1), :]
            column = jnp.sum(jnp.where(eye, line, 0.0), axis=1, keepdims=True)
            wc[e, span(n, share), :] = jnp.broadcast_to(column, (share, LANES))
    each(0, nt * width, shares)

    with jax.named_scope('gather'):
        settle(xr.at[0:nt - 1], gsem.at[1])

    def product(a, e, i):
        total = jnp.zeros((plane, hidden), F32)
        for o in range(nt):
            left = xr[o, i].reshape(plane, cols)
            total += matmul(left, served[a][e, o * cols:(o + 1) * cols, :])
        return total * d_model ** (-0.5)

    with jax.named_scope('wait_gate'):
        settle(ws.at[0, 0:experts - per], wrecv.at[0])
    with jax.named_scope('wait_up'):
        settle(ws.at[1, 0:experts - per], wrecv.at[1])

    def activate(i):
        for e in range(per):
            v = product(0, e, i)
            value = v / (1.0 + jnp.exp(-v)) * product(1, e, i)
            value = value * wc[e, span(i, plane), 0:1]
            hs[span(i, plane), e * hidden:(e + 1) * hidden] = value.astype(BF16)
    pl.when(outer)(lambda: send_down(0, parts))
    with jax.named_scope('activate'):
        each(0, nt, activate)

    hidden_scale = (hidden * nt) ** (-0.5)
    blocks = pieces // parts
    quarter = pieces // GROUPS
    wide_blocks = blocks // GROUPS
    def piece_at(n):
        j, r = (n - quarter) // wide_blocks, lax.rem(n, wide_blocks)
        first = n < quarter
        h = jnp.where(first, n // wide_blocks, jnp.where(outer, lax.rem(j, parts), j // 3))
        turn = jnp.where(outer, j // parts, lax.rem(j, 3))
        turn = jnp.where((turn < 2) & (h > 0) & jnp.logical_not(outer), 1 - turn, turn)
        far = jnp.where(lower, GROUPS - turn, turn - 1)
        z = jnp.where(first, g, jnp.where(turn == 0, g ^ 1, far))
        return (z * wide_blocks + r) * parts + h

    def multiply(n):
        c = piece_at(n)
        h = lax.rem(c, parts)
        for q in range(joint):
            s = c // parts * joint + q

            @pl.when(s != f)
            def _():
                with jax.named_scope('wait_piece'):
                    down_copy(h, f, s).wait_recv()
        value = jnp.zeros((nt * plane, LANES), F32)
        for e in range(per):
            value += matmul(
                hs[:, e * hidden:(e + 1) * hidden], down_out[e, span(c, LANES), :], ((1,), (1,)))
        ps[c] = (value * hidden_scale).astype(BF16).reshape(2, nt // 2, plane, LANES)
        partial_copy(c, t + 1).start()

    def reduce(n):
        c = piece_at(n)
        with jax.named_scope('wait_partial'):
            partial_copy(c, t).wait_recv()
        total = ps[c, lax.rem(t, 2)].astype(F32) + pr[c].astype(F32)
        qs[c] = total.astype(BF16).reshape(crews, share, LANES)
        each(1, crews, lambda k: crew_copy(c, crew(k), crew(0)).start())

    def give_back(n):
        c = piece_at(n)
        with jax.named_scope('wait_mate'):
            settle(qs.at[c, 0:crews - 1], qrecv.at[c])
        total = qs[c, crew(0)].astype(F32)
        for k in range(1, crews):
            total += qr[crew(k), c].astype(F32)
        rs[c] = total.astype(BF16)
        owner = c // per_owner
        local = (home == g) & (owner == t)

        @pl.when(local)
        def _():
            ret[lax.rem(c, per_owner), span(g * split + rest, share), :] = rs[c]

        pl.when(jnp.logical_not(crossing) | (n >= late))(lambda: send_back(n))

    crossing = outer & ((home < GROUPS // 2) != (g < GROUPS // 2))

    def send_back(n):
        c = piece_at(n)
        owner = c // per_owner

        @pl.when((home != g) | (owner != t))
        def _():
            return_copy(c, home * width + m, owner, g * split + rest).start()

    late = pieces - wide_blocks

    def step(n):
        multiply(n)
        pl.when(n >= PAIR_LAG)(lambda: reduce(n - PAIR_LAG))
        pl.when(n >= CREW_LAG)(lambda: give_back(n - CREW_LAG))
    each(0, late, step)
    each(late - PAIR_LAG, late, reduce)
    each(late, pieces, multiply)
    each(late, pieces, reduce)
    each(late - CREW_LAG, pieces, give_back)
    pl.when(crossing)(lambda: each(0, late, send_back))

    own_share = pieces - per_owner

    @pl.when(home == g)
    def _():
        settle(ret.at[:, 0:GROUPS * slots - share], rsem.at[1])
        settle(rs.at[0:own_share], rsem.at[0])

    @pl.when(home != g)
    def _():
        settle(ret, rsem.at[1])
        settle(rs, rsem.at[0])

    for a in range(3):
        settle(ws.at[a, 0:experts - per], wsend.at[a])
    settle(xs.at[0:GROUPS - 1], xsem.at[0])
    settle(vs.at[0:GROUPS - 1], vsem.at[0])
    settle(xr.at[t, :, 0:width - 1], msem.at[0])
    settle(vr.at[:, 0:width - 1], nsem.at[0])
    settle(xr.at[0:nt - 1], gsem.at[0])
    settle(pr, psend)
    settle(qs.at[:, 0:crews - 1], qsend)


def finish_kernel(
    ids_t, ret, gate, up, down, gate_out, up_out, down_out, combined, result, sem, *, per_group
):
    outs = [
        pltpu.make_async_copy(source, target, sem.at[a])
        for a, (source, target) in enumerate(((gate, gate_out), (up, up_out), (down, down_out)))
    ]
    for copy in outs:
        copy.start()
    chunks, slots, width = ret.shape
    chosen = placement(ids_t, per_group, slots // GROUPS)
    for i in range(chunks):
        value = matmul(chosen, ret[i], ((0,), (0,)))
        result[:, i * width:(i + 1) * width] = value.astype(BF16)
    last = pltpu.make_async_copy(result, combined, sem.at[3])
    last.start()
    for copy in outs:
        copy.wait()
    last.wait()


def body(nf, nt, tokens, route_ids, route_weights, norm_gain, gate_weight, up_weight, down_weight):
    experts, rows, hidden = gate_weight.shape
    n_tok, d_model = tokens.shape
    per = experts // nf
    cols = d_model // nt
    slots = n_tok // route_ids.shape[1]
    width = nf // GROUPS
    per_group = experts // GROUPS
    lines = max(8, per_group)
    crews = nt // 2 * width
    split = nt // GROUPS
    share = slots // split
    parts = max(1, rows // LANES)
    pieces = d_model // LANES
    per_owner = cols // LANES
    shape = (per, nf * rows, hidden)
    vmem, anywhere = pl.BlockSpec(memory_space=pltpu.VMEM), pl.BlockSpec(memory_space=pl.ANY)
    dma = pltpu.SemaphoreType.DMA
    ids_t, weights_t = route_ids.T, route_weights.T
    *served, ret = pl.pallas_call(
        functools.partial(kernel, nf, nt),
        out_shape=[pltpu.VMEM(shape, BF16)] * 3
        + [pltpu.VMEM((per_owner, GROUPS * slots, LANES), BF16)],
        in_specs=[anywhere] * 7,
        out_specs=[vmem] * 4,
        scratch_shapes=[
            pltpu.VMEM((n_tok, d_model), BF16),
            pltpu.VMEM(ids_t.shape, I32),
            pltpu.VMEM(weights_t.shape, F32),
            pltpu.VMEM((1, rows), F32),
            pltpu.VMEM((2, experts, rows, hidden), F32),
            pltpu.VMEM((3, experts, rows, hidden), BF16),
            pltpu.VMEM((GROUPS, split, share, cols), BF16),
            pltpu.VMEM((GROUPS, lines, n_tok), F32),
            pltpu.VMEM((nt, nt, width, share, cols), BF16),
            pltpu.VMEM((GROUPS, width, lines, n_tok), F32),
            pltpu.VMEM((per, nf * slots, LANES), F32),
            pltpu.VMEM((nf * slots, per * hidden), BF16),
            pltpu.VMEM((pieces, 2, nt // 2, width * share, LANES), BF16),
            pltpu.VMEM((pieces, nt // 2, width * share, LANES), BF16),
            pltpu.VMEM((pieces, crews, share, LANES), BF16),
            pltpu.VMEM((crews, pieces, share, LANES), BF16),
            pltpu.VMEM((pieces, share, LANES), BF16),
            dma((4,)), dma((nf,)), dma((3,)), dma((2,)), dma((parts, nf)),
            dma((2,)), dma((2,)), dma((2,)), dma((2,)), dma((2,)),
            dma, dma((pieces,)), dma, dma((pieces,)), dma((2,)),
        ],
        compiler_params=pltpu.CompilerParams(
            collective_id=0, has_side_effects=True, vmem_limit_bytes=54 * 1024 * 1024
        ),
    )(tokens, ids_t, weights_t, norm_gain[None, :], gate_weight, up_weight, down_weight)
    out = jax.ShapeDtypeStruct(shape, BF16)
    return pl.pallas_call(
        functools.partial(finish_kernel, per_group=per_group),
        out_shape=(out, out, out, jax.ShapeDtypeStruct((n_tok, cols), BF16)),
        in_specs=[vmem] * 5,
        out_specs=(anywhere,) * 4,
        scratch_shapes=[pltpu.VMEM((n_tok, cols), BF16), dma((4,))],
        compiler_params=pltpu.CompilerParams(vmem_limit_bytes=16 * 1024 * 1024),
    )(ids_t, ret, *served)


def solution(mesh):
    split = P(None, "fs", "tp")
    served = P("fs", None, "tp")
    return jax.shard_map(
        functools.partial(body, mesh.shape["fs"], mesh.shape["tp"]),
        mesh=mesh,
        in_specs=(P("fs", None), P("fs", None), P("fs", None), P("fs"), split, split, split),
        out_specs=(served, served, served, P("fs", "tp")),
        check_vma=False,
    )
```
